256 devices in a mesh: grp: 2 (over y), sp: 16 (over z), tp: 8 (over x, core).
Axes of the slice: x: 4, y: 2, z: 16, core: 2. Of those that a mesh axis runs over, the one named last changes fastest.
The devices are a block of a 4x16x16 slice.
Arguments:
- queries: bfloat16 [16384, 2048], P(('grp', 'sp'), 'tp'), parts along dimension 0, may hold values from -6 to 6
- key_vectors: bfloat16 [16384, 2048], P(('grp', 'sp'), 'tp'), parts along dimension 0, may hold values from -6 to 6
- value_vectors: bfloat16 [16384, 2048], P(('grp', 'sp'), 'tp'), parts along dimension 0, may hold values from -6 to 6
- forget_sums: float32 [16384, 16], P(('grp', 'sp'), 'tp'), parts along dimension 0, may hold values from -8192 to 0, as said below
- residual: bfloat16 [16384, 2048], P(('grp', 'sp'), 'tp'), parts along dimension 0, may hold values from -20 to 20
- query_gain: float32 [128], replicated, may hold values from 0.5 to 5
- key_gain: float32 [128], replicated, may hold values from 0.5 to 5
- out_weight: bfloat16 [2048, 2048], P(None, 'tp'), may hold values from -0.125 to 0.125
- norm_gain: float32 [2048], replicated, may hold values from 0.1 to 1.9
- gate_weight: bfloat16 [2048, 5504], P('sp', 'tp'), may hold values from -0.125 to 0.125
- up_weight: bfloat16 [2048, 5504], P('sp', 'tp'), may hold values from -0.125 to 0.125
- down_weight: bfloat16 [2048, 5504], P('sp', 'tp'), may hold values from -0.078125 to 0.078125
Outputs:
- layer_output: bfloat16 [16384, 2048], P(('grp', 'sp'), 'tp'), parts along dimension 0
The draws below stay inside these ranges and needn't reach their ends.
There are 2 independent parts, one for each index of `grp`. The reference program is written for one: setup_inputs(seed, part) draws one part's arguments, and reference() takes and returns one part's arrays. A program takes and returns all parts, laid end to end along the dimension named above; an argument that names none is the same for every part. Nothing has to cross between parts.
Inputs may be any that keep to these rules, and one draw needn't show every extreme that they name: `forget_sums`: along positions each head's values never rise.
All inputs are finite; a program needn't handle non-finite values.
Results may differ from the reference program's by a relative error of at most 0.011.
Values may be sent and summed in bfloat16 or wider, within the bound.
A program may use at most 128 MiB of HBM per device.

```python
import math
import jax
import jax.numpy as jnp
from jax import lax

D = 2048
HEADS = 16
HEAD = 128
FF = 5504
TOK_DEV = 512
TOKENS = 8192
N_TP = 8


def paired_rows(key):
    base = jax.random.fold_in(key, 101)
    first, second = jax.random.split(base, 2)
    width = HEADS * HEAD
    query_rows = jax.random.normal(first, (TOKENS, width), jnp.float32)
    key_rows = jax.random.normal(second, (TOKENS, width), jnp.float32)
    return (jnp.clip(query_rows, -6.0, 6.0), jnp.clip(key_rows, -6.0, 6.0))


def draw_queries(key, part):
    return paired_rows(key)[0].astype(jnp.bfloat16)


def draw_key_vectors(key, part):
    return paired_rows(key)[1].astype(jnp.bfloat16)


def draw_gain_common(key, salt):
    inner = jax.random.fold_in(key, salt)
    return jnp.exp(jax.random.uniform(inner, (HEAD,), jnp.float32, math.log(0.5), math.log(2.0)))


def draw_query_gain(key, part):
    return draw_gain_common(key, 201)


def draw_key_gain(key, part):
    return draw_gain_common(key, 202)


def draw_forget_sums(key, part):
    base = jax.random.fold_in(key, 301)
    parts = jax.random.split(base, 7)
    order = jax.random.permutation(parts[0], HEADS)
    fast = order < HEADS // 2
    fast_rate = jnp.exp(jax.random.uniform(parts[1], (HEADS,), jnp.float32, math.log(1.0 / 80.0), math.log(1.0 / 30.0)))
    slow_rate = jnp.exp(jax.random.uniform(parts[2], (HEADS,), jnp.float32, math.log(0.5), math.log(2.0))) * (0.4 / TOKENS)
    rate = jnp.where(fast, fast_rate, slow_rate)
    noise = jnp.exp(jax.random.uniform(parts[3], (TOKENS, HEADS), jnp.float32, math.log(0.5), math.log(2.0)))
    block_factor = jnp.exp(jax.random.uniform(parts[4], (TOKENS // TOK_DEV,), jnp.float32, math.log(0.5), math.log(2.0)))
    block_factor = jnp.repeat(block_factor, TOK_DEV)
    log_gates = -rate[None, :] * noise * block_factor[:, None]
    places = jax.random.randint(parts[5], (3,), 0, TOKENS)
    drops = jnp.log(jax.random.uniform(parts[6], (3, HEADS), jnp.float32, 0.5, 0.8))
    marks = (jnp.arange(TOKENS)[:, None] == places[None, :]).astype(jnp.float32)
    log_gates = log_gates + jnp.dot(marks, drops)
    return jnp.cumsum(log_gates, axis=0)


def draw_residual(key, part):
    base = jax.random.fold_in(key, 401)
    parts = jax.random.split(base, 3)
    column_scale = jnp.exp(jnp.linspace(math.log(0.4), math.log(3.0), D)) * jnp.exp(jax.random.uniform(parts[0], (D,), jnp.float32, math.log(0.7), math.log(1.4)))
    rows = jnp.clip(jax.random.normal(parts[2], (TOKENS, D), jnp.float32), -5.0, 5.0)
    return jnp.clip(rows * column_scale[None, :], -20.0, 20.0).astype(jnp.bfloat16)


def level_of(stream_key, dims, pieces, smallest, top_value):
    def one(axis_at, shards_of):
        draws = jax.random.uniform(jax.random.fold_in(jax.random.fold_in(stream_key, 6), axis_at), (shards_of,), jnp.float32, smallest / len(pieces), top_value / len(pieces))
        return jnp.repeat(jnp.exp(draws), dims[axis_at] // shards_of).reshape((-1,) + (1,) * (len(dims) - axis_at - 1))

    level = one(*pieces[0])
    for cut in pieces[1:]:
        level = level * one(*cut)
    return level


def scatter_about(rng, extent, deviation, limit, shards=(), kind=jnp.bfloat16):
    level = level_of(rng, extent, shards, -0.22, 0.18) if shards else 1.0
    drawn = jax.random.normal(rng, extent, jnp.float32) * deviation * level
    return jnp.minimum(jnp.maximum(drawn, -limit), limit).astype(kind)


def setup_inputs(seed: int = 0, part: int = 0) -> dict:
    key_of = jax.random.split(jax.random.key(seed), 13)
    own_keys = jax.random.split(jax.random.fold_in(key_of[12], part), 13)
    queries = draw_queries(jax.random.fold_in(jax.random.fold_in(key_of[12], part), 71), part)
    key_vectors = draw_key_vectors(jax.random.fold_in(jax.random.fold_in(key_of[12], part), 71), part)
    value_vectors = scatter_about(own_keys[2], (TOKENS, HEADS * HEAD), 1.0, 6.0, ((0, 16), (1, 8)))
    forget_sums = draw_forget_sums(jax.random.fold_in(jax.random.fold_in(key_of[12], part), 71), part)
    residual = draw_residual(jax.random.fold_in(jax.random.fold_in(key_of[12], part), 71), part)
    query_gain = draw_query_gain(jax.random.fold_in(key_of[12], 71), part)
    key_gain = draw_key_gain(jax.random.fold_in(key_of[12], 71), part)
    out_weight = scatter_about(key_of[7], (HEADS * HEAD, D), (HEADS * HEAD) ** -0.5, 0.125, ((1, 8),))
    norm_gain = jnp.clip(1.0 + 0.18 * jax.random.normal(key_of[8], (D,), jnp.float32), 0.1, 1.9)
    gate_weight = scatter_about(key_of[9], (D, FF), D ** -0.5, 0.125, ((0, 16), (1, 8)))
    up_weight = scatter_about(key_of[10], (D, FF), D ** -0.5, 0.125, ((0, 16), (1, 8)))
    down_weight = scatter_about(key_of[11], (D, FF), FF ** -0.5, 0.078125, ((0, 16), (1, 8)))
    return {"queries": queries, "key_vectors": key_vectors, "value_vectors": value_vectors, "forget_sums": forget_sums, "residual": residual, "query_gain": query_gain, "key_gain": key_gain, "out_weight": out_weight, "norm_gain": norm_gain, "gate_weight": gate_weight, "up_weight": up_weight, "down_weight": down_weight}


eps = 1e-06

def head_norm(rows_in, gain):
    count = rows_in.shape[0]
    split = rows_in.reshape(count, -1, HEAD).astype(jnp.float32)
    factor = lax.rsqrt(lax.optimization_barrier(jnp.mean(split * split, axis=2, keepdims=True)) + eps)
    return (split * factor * gain).astype(jnp.bfloat16)

def reference(queries, key_vectors, value_vectors, forget_sums, residual, query_gain, key_gain, out_weight, norm_gain, gate_weight, up_weight, down_weight):
    query_norm = head_norm(queries, query_gain)
    key_norm = lax.optimization_barrier(head_norm(key_vectors, key_gain)).astype(jnp.float32)
    values = value_vectors.reshape(TOKENS, HEADS, HEAD).astype(jnp.float32)
    biases = forget_sums.T
    block = math.gcd(TOKENS, 512)
    key_pos = jnp.arange(TOKENS, dtype=jnp.int32)
    factor = 1.0 / math.sqrt(HEAD)

    def attend(index):
        first = index * block
        query_block = lax.optimization_barrier(lax.dynamic_slice_in_dim(query_norm, first, block, 0)).astype(jnp.float32)
        scores = jnp.einsum('qhd,khd->hqk', query_block, key_norm) * factor
        query_bias = lax.dynamic_slice_in_dim(biases, first, block, 1)
        scores = scores + query_bias[:, :, None] - biases[:, None, :]
        query_pos = first + jnp.arange(block, dtype=jnp.int32)
        allowed = key_pos[None, :] <= query_pos[:, None]
        scores = jnp.where(allowed[None], scores, -jnp.inf)
        top = lax.optimization_barrier(jnp.max(scores, axis=2, keepdims=True))
        raised = jnp.exp(scores - top)
        totals = lax.optimization_barrier(jnp.sum(raised, axis=2))
        weights = lax.optimization_barrier(raised.astype(jnp.bfloat16)).astype(jnp.float32)
        summed = jnp.einsum('hqk,khd->qhd', weights, values)
        return (summed / totals.T[:, :, None]).astype(jnp.bfloat16)
    attended = lax.map(attend, jnp.arange(TOKENS // block, dtype=jnp.int32)).reshape(TOKENS, HEADS * HEAD)
    projected = jnp.dot(attended, out_weight, preferred_element_type=jnp.float32)
    middle = (residual.astype(jnp.float32) + projected).astype(jnp.bfloat16)
    whole = middle.astype(jnp.float32)
    normed = (whole * lax.rsqrt(lax.optimization_barrier(jnp.mean(whole * whole, axis=1, keepdims=True)) + eps) * norm_gain).astype(jnp.bfloat16)
    gate = jnp.dot(normed, gate_weight, preferred_element_type=jnp.float32)
    upward = jnp.dot(normed, up_weight, preferred_element_type=jnp.float32)
    hidden = (jax.nn.silu(gate) * upward).astype(jnp.bfloat16)
    width = FF // N_TP

    def add_block(index, total):
        start = (index * width).astype(jnp.int32)
        hidden_part = lax.dynamic_slice_in_dim(hidden, start, width, 1)
        weight_part = lax.dynamic_slice_in_dim(down_weight, start, width, 1)
        partial_value = lax.dot_general(hidden_part, weight_part, (((1,), (1,)), ((), ())), preferred_element_type=jnp.float32)
        rounded = lax.optimization_barrier(partial_value.astype(jnp.bfloat16))
        return total + rounded.astype(jnp.float32)
    down = lax.fori_loop(0, N_TP, add_block, jnp.zeros((TOKENS, D), jnp.float32))
    return (whole + down).astype(jnp.bfloat16)
```

```python
import functools
import math

import jax
import jax.numpy as jnp
from jax import lax
from jax.experimental import pallas as pl
from jax.experimental.pallas import tpu as pltpu
from jax.sharding import PartitionSpec as P

MESH = pl.DeviceIdType.MESH
HEAD = 128
EPS = 1e-06
LOW = -1e30
LOG2E = 1.4426950408889634


def remote(src, dst, send, recv, device):
    return pltpu.make_async_remote_copy(
        src_ref=src, dst_ref=dst, send_sem=send, recv_sem=recv, device_id=device, device_id_type=MESH
    )


def arrived(ref, sem, device):
    remote(ref, ref, sem, sem, device).wait_recv()


def left_over(ref, sem, device):
    remote(ref, ref, sem, sem, device).wait_send()


class Row:
    def __init__(self, t, size):
        self.t = t
        self.left = lax.rem(t + size - 2, size)
        self.right = lax.rem(t + 2, size)
        self.opp = lax.rem(t + size // 2, size)
        self.core = lax.rem(t, 2)

    @staticmethod
    def other(t):
        return t + 1 - 2 * lax.rem(t, 2)


def row_gather(row, buf, send, recv):
    half = buf.shape[1] // 2
    t, left, right, opp = row.t, row.left, row.right, row.opp
    other = Row.other
    to_left, to_right, to_other = {"tp": left}, {"tp": right}, {"tp": other(t)}
    first, second = pl.ds(0, half), pl.ds(half, half)
    sent = []

    def go(ref, at, device):
        copy = remote(ref, ref, send.at[at], recv.at[at], device)
        copy.start()
        sent.append(copy)

    go(buf.at[t], 0, to_right)
    go(buf.at[t], 1, to_left)
    go(buf.at[t], 2, to_other)
    arrived(buf.at[left], recv.at[0], to_left)
    go(buf.at[left, first], 3, to_right)
    go(buf.at[left], 4, to_other)
    arrived(buf.at[right], recv.at[1], to_right)
    go(buf.at[right, second], 5, to_left)
    go(buf.at[right], 6, to_other)
    arrived(buf.at[opp, first], recv.at[3], to_left)
    go(buf.at[opp, first], 7, to_other)
    arrived(buf.at[opp, second], recv.at[5], to_right)
    go(buf.at[opp, second], 8, to_other)
    arrived(buf.at[other(t)], recv.at[2], to_other)
    arrived(buf.at[other(left)], recv.at[4], to_other)
    arrived(buf.at[other(right)], recv.at[6], to_other)
    arrived(buf.at[other(opp), first], recv.at[7], to_other)
    arrived(buf.at[other(opp), second], recv.at[8], to_other)
    for copy in sent:
        copy.wait_send()


def normed(rows, gain):
    square = jnp.mean(rows * rows, axis=-1, keepdims=True)
    return rows * lax.rsqrt(square + EPS) * gain


def attention_kernel(
    n_sp,
    n_tp,
    q_ref,
    k_ref,
    v_ref,
    f_ref,
    res_ref,
    ow_ref,
    qg_ref,
    kg_ref,
    out_ref,
    qbuf,
    kv,
    fbuf,
    kn,
    obuf,
    att,
    mid,
    send_a,
    recv_a,
    send_b,
    recv_b,
    send_c,
    recv_c,
    send_o,
    recv_o,
    send_g,
    recv_g,
    out_sem,
):
    s = lax.axis_index("sp")
    t = lax.axis_index("tp")
    row = Row(t, n_tp)
    other = Row.other
    left, right, opp = row.left, row.right, row.opp
    sub = qbuf.shape[1]
    per = n_sp // 4

    def row_of(head):
        return lax.rem(head, per) * 4 + head // per

    def head_of(r):
        return lax.rem(r, 4) * per + r // 4

    my_head = head_of(s)
    source = my_head // 2

    barrier = pltpu.get_barrier_semaphore()

    def hello(device):
        pl.semaphore_signal(barrier, inc=1, device_id=device, device_id_type=MESH)

    for peer in (left, right, other(t)):
        hello({"tp": peer})

    @pl.loop(0, n_sp)
    def _(r):
        @pl.when(r != s)
        def _():
            hello({"sp": r, "tp": t})

        @pl.when(jnp.logical_or(r != s, t != source))
        def _():
            hello({"sp": r, "tp": source})

    own = jnp.logical_or(row_of(2 * t) == s, row_of(2 * t + 1) == s)
    pl.semaphore_wait(barrier, 3 + n_sp - 1 + 2 * n_tp - own.astype(jnp.int32))

    def pieces(u, hi):
        there = lax.rem(t + u, n_tp)
        rows, cols = pl.ds(there * sub, sub), pl.ds(hi * HEAD, HEAD)
        return there, (
            (q_ref.at[rows, cols], qbuf.at[s], 0, recv_a.at[n_sp]),
            (f_ref.at[hi], fbuf.at[s], 1, recv_a.at[n_sp + 1]),
            (k_ref.at[rows, cols], kv.at[s, there, 0], 2, recv_a.at[s]),
            (v_ref.at[rows, cols], kv.at[s, there, 1], 3, recv_a.at[s]),
        )

    def each_piece(act, start):
        @pl.loop(0, n_tp)
        def _(u):
            for hi in range(2):
                r = row_of(2 * t + hi)
                there, list_of = pieces(u, hi)
                mine = jnp.logical_and(r == s, there == t)

                @pl.when(jnp.logical_not(mine))
                def _():
                    for src, dst, i, sem in list_of:
                        act(remote(src, dst, send_a.at[hi, u, i], sem, {"sp": r, "tp": there}))

                if start:

                    @pl.when(mine)
                    def _():
                        for src, dst, _, sem in list_of:
                            pltpu.make_async_copy(src, dst, sem).start()

    each_piece(lambda c: c.start(), True)

    to_left, to_right, to_other = {"tp": left}, {"tp": right}, {"tp": other(t)}

    def at_step(j):
        d = (j + 1) // 2
        return lax.rem(s + n_sp + jnp.where(lax.rem(j, 2) == 1, d, -d), n_sp)

    def stage_one(j):
        b = at_step(j)
        arrived(kv.at[b, t], recv_a.at[b], to_other)
        piece = kv.at[b, t]
        remote(piece, piece, send_b.at[0], recv_b.at[0, b], to_right).start()
        remote(piece, piece, send_b.at[1], recv_b.at[1, b], to_left).start()
        remote(piece, piece, send_b.at[2], recv_c.at[0], to_other).start()

    def stage_two(j):
        b = at_step(j)
        arrived(kv.at[b, left], recv_b.at[0, b], to_left)
        piece, part = kv.at[b, left], kv.at[b, left, 0]
        remote(part, part, send_b.at[3], recv_b.at[2, b], to_right).start()
        remote(piece, piece, send_c.at[0], recv_c.at[1], to_other).start()
        arrived(kv.at[b, right], recv_b.at[1, b], to_right)
        piece, part = kv.at[b, right], kv.at[b, right, 1]
        remote(part, part, send_b.at[4], recv_b.at[3, b], to_left).start()
        remote(piece, piece, send_c.at[1], recv_c.at[2], to_other).start()

    def stage_three(j):
        b = at_step(j)
        arrived(kv.at[b, opp, 0], recv_b.at[2, b], to_left)
        part = kv.at[b, opp, 0]
        remote(part, part, send_c.at[2], recv_c.at[3], to_other).start()
        arrived(kv.at[b, opp, 1], recv_b.at[3, b], to_right)
        part = kv.at[b, opp, 1]
        remote(part, part, send_c.at[3], recv_c.at[4], to_other).start()

    lag = 2

    @pl.loop(0, n_sp + 2 * lag)
    def _(j):
        @pl.when(j < n_sp)
        def _():
            stage_one(j)

        @pl.when(jnp.logical_and(j >= lag, j < n_sp + lag))
        def _():
            stage_two(j - lag)

        @pl.when(j >= 2 * lag)
        def _():
            stage_three(j - 2 * lag)

    arrived(kv.at[:, other(t)], recv_c.at[0], to_other)
    arrived(kv.at[:, other(left)], recv_c.at[1], to_other)
    arrived(kv.at[:, other(right)], recv_c.at[2], to_other)
    arrived(kv.at[:, other(opp), 0], recv_c.at[3], to_other)
    arrived(kv.at[:, other(opp), 1], recv_c.at[4], to_other)
    arrived(qbuf, recv_a.at[n_sp], to_other)
    arrived(fbuf, recv_a.at[n_sp + 1], to_other)

    width = n_tp * sub

    @pl.loop(0, n_sp)
    def _(b):
        rows = kv[b, :, 0].reshape(width, HEAD).astype(jnp.float32)
        kn[b] = normed(rows, kg_ref[...]).astype(jnp.bfloat16)

    group = 4
    tall, wide = group * sub, group * width
    factor = LOG2E / math.sqrt(HEAD)

    def bias_row(c, base):
        parts = []
        for b in range(group):
            slab = fbuf[c * group + b]
            for lane in range(width // HEAD):
                parts.append(slab[lane : lane + 1])
        return (base - jnp.concatenate(parts, axis=1)) * LOG2E

    @pl.loop(0, n_sp // group)
    def _(step):
        i = n_sp // group - 1 - step
        q = qbuf[pl.ds(i * group, group)].reshape(tall, HEAD).astype(jnp.float32)
        q = normed(q, qg_ref[...]).astype(jnp.bfloat16)
        base = fbuf[i * group, 0:1, 0:1]

        def visit(c, state, masked):
            top, total, acc = state
            keys = kn[pl.ds(c * group, group)].reshape(wide, HEAD)
            scores = lax.dot_general(q, keys, (((1,), (1,)), ((), ())), preferred_element_type=jnp.float32)
            scores = scores * factor + bias_row(c, base)
            if masked:
                line = lax.broadcasted_iota(jnp.int32, (tall, wide), 0)
                place = (line // sub) * width + t * sub + lax.rem(line, sub)
                scores = jnp.where(lax.broadcasted_iota(jnp.int32, (tall, wide), 1) <= place, scores, LOW)
            high = jnp.maximum(top, jnp.max(scores, axis=1, keepdims=True))
            raised = jnp.exp2(scores - high)
            shrink = jnp.exp2(top - high)
            total = total * shrink + jnp.sum(raised, axis=1, keepdims=True)
            vals = kv[pl.ds(c * group, group), :, 1].reshape(wide, HEAD)
            acc = acc * shrink + jnp.dot(raised.astype(jnp.bfloat16), vals, preferred_element_type=jnp.float32)
            return high, total, acc

        state = (
            jnp.full((tall, 1), LOW, jnp.float32),
            jnp.zeros((tall, 1), jnp.float32),
            jnp.zeros((tall, HEAD), jnp.float32),
        )
        state = visit(i, state, True)
        _, total, acc = lax.fori_loop(0, i, lambda c, st: visit(c, st, False), state)
        obuf[pl.ds(i * group, group)] = (acc / total).astype(jnp.bfloat16).reshape(group, sub, HEAD)

        @pl.loop(0, group)
        def _(n):
            r = i * group + n
            cols = pl.ds(pl.multiple_of(my_head * HEAD, HEAD), HEAD)

            @pl.when(r != s)
            def _():
                remote(obuf.at[r], att.at[t, :, cols], send_o.at[r], recv_o, {"sp": r, "tp": t}).start()

            @pl.when(r == s)
            def _():
                att[t, :, cols] = obuf[r]

    def o_wait(r):
        @pl.when(r != s)
        def _():
            left_over(obuf.at[r], send_o.at[r], {"sp": r, "tp": t})

    pl.loop(0, n_sp)(o_wait)
    arrived(att.at[t, :, pl.ds(0, (n_sp - 1) * HEAD)], recv_o, to_other)

    row_gather(row, att, send_g.at[0], recv_g.at[0])
    total_rows = n_tp * sub
    span = 256

    @pl.loop(0, total_rows // span)
    def _(m):
        rows = pl.ds(m * span, span)
        lhs = att[pl.ds(m * (span // sub), span // sub)].reshape(span, att.shape[2])
        product = jnp.dot(lhs, ow_ref[...], preferred_element_type=jnp.float32)
        mid[t, rows] = (res_ref[rows].astype(jnp.float32) + product).astype(jnp.bfloat16)

    row_gather(row, mid, send_g.at[1], recv_g.at[1])
    out = pltpu.make_async_copy(mid, out_ref, out_sem)
    out.start()

    each_piece(lambda c: c.wait_send(), False)
    left_over(kv.at[:, t], send_b.at[0], to_right)
    left_over(kv.at[:, t], send_b.at[1], to_left)
    left_over(kv.at[:, t], send_b.at[2], to_other)
    left_over(kv.at[:, left, 0], send_b.at[3], to_right)
    left_over(kv.at[:, right, 1], send_b.at[4], to_left)
    left_over(kv.at[:, left], send_c.at[0], to_other)
    left_over(kv.at[:, right], send_c.at[1], to_other)
    left_over(kv.at[:, opp, 0], send_c.at[2], to_other)
    left_over(kv.at[:, opp, 1], send_c.at[3], to_other)
    out.wait()


def feed_forward_kernel(
    n_sp,
    n_tp,
    mid_ref,
    w_ref,
    gain_ref,
    out_ref,
    mid,
    wg,
    wu,
    wd,
    nrm,
    hid,
    part,
    pair,
    total,
    landed,
    load_sem,
    send_p,
    recv_p,
    send_r,
    recv_r,
):
    t = lax.axis_index("tp")
    row = Row(t, n_tp)
    other = Row.other
    left, right, opp, core = row.left, row.right, row.opp, row.core
    ff = wg.shape[0]
    cols = mid.shape[2]
    depth = w_ref.shape[2]
    rows = mid.shape[1]

    loads = [pltpu.make_async_copy(mid_ref, mid, load_sem.at[0])]
    for i, w in enumerate((wg, wu, wd)):
        for z in range(n_sp):
            loads.append(
                pltpu.make_async_copy(
                    w_ref.at[z, pl.ds(i * ff, ff)], w.at[:, pl.ds(z * depth, depth)], load_sem.at[1 + i * n_sp + z]
                )
            )
    for load in loads:
        load.start()

    barrier = pltpu.get_barrier_semaphore()
    for peer in (left, right, opp, other(t)):
        pl.semaphore_signal(barrier, inc=1, device_id={"tp": peer}, device_id_type=MESH)
    pl.semaphore_wait(barrier, 4)

    loads[0].wait()
    span = 128

    @pl.loop(0, rows // span)
    def _(m):
        at = pl.ds(m * span, span)
        blocks = [mid[u, at].astype(jnp.float32) for u in range(n_tp)]
        square = sum(jnp.sum(b * b, axis=1, keepdims=True) for b in blocks) / (n_tp * cols)
        scale = lax.rsqrt(square + EPS)
        for u in range(n_tp):
            nrm[at, pl.ds(u * cols, cols)] = (blocks[u] * scale * gain_ref[u]).astype(jnp.bfloat16)

    for load in loads[1:]:
        load.wait()
    tall = 256

    @pl.loop(0, rows // tall)
    def _(m):
        at = pl.ds(m * tall, tall)
        across = (((1,), (1,)), ((), ()))
        gate = lax.dot_general(nrm[at], wg[...], across, preferred_element_type=jnp.float32)
        up = lax.dot_general(nrm[at], wu[...], across, preferred_element_type=jnp.float32)
        hid[at] = (gate / (1.0 + jnp.exp(-gate)) * up).astype(jnp.bfloat16)

    to_other = {"tp": other(t)}
    chips = (opp, right, left, t)

    def add(k):
        arrived(pair.at[k], recv_p.at[k], to_other)
        mine = part[k, core].astype(jnp.float32) + pair[k].astype(jnp.float32)
        if k < 3:
            total[k] = mine.astype(jnp.bfloat16)
            remote(total.at[k], landed.at[k], send_r.at[k], recv_r.at[k], {"tp": chips[k]}).start()
            return None
        return mine

    for k in range(4):
        base = (chips[k] - core) * cols
        for side in range(2):
            at = pl.ds(pl.multiple_of(base + side * cols, cols), cols)
            part[k, side] = jnp.dot(hid[...], wd[:, at], preferred_element_type=jnp.float32).astype(jnp.bfloat16)
        remote(part.at[k, 1 - core], pair.at[k], send_p.at[k], recv_p.at[k], to_other).start()
        if k > 0:
            add(k - 1)
    mine = add(3) + mid[t].astype(jnp.float32)
    for k in (1, 2, 0):
        arrived(landed.at[k], recv_r.at[k], to_other)
        mine = mine + landed[k].astype(jnp.float32)
    out_ref[...] = mine.astype(jnp.bfloat16)
    for k in range(4):
        left_over(part.at[k, 1 - core], send_p.at[k], to_other)
    for k in range(3):
        left_over(total.at[k], send_r.at[k], {"tp": chips[k]})


def local(n_sp, n_tp, q, k, v, f, res, qg, kg, ow, ng, gw, uw, dw):
    rows, cols = q.shape
    sub = rows // n_tp
    hbm = pl.BlockSpec(memory_space=pltpu.HBM)
    vmem = pl.BlockSpec(memory_space=pltpu.VMEM)
    dma = pltpu.SemaphoreType.DMA
    flat = jnp.concatenate((gw, uw, dw), axis=1).T
    w = lax.all_gather(flat, "sp", axis=0)
    f = jnp.pad(f.T.reshape(2, rows // HEAD, HEAD), ((0, 0), (0, 8 - rows // HEAD), (0, 0)))
    bf = jnp.bfloat16
    width = n_sp * HEAD
    mid = pl.pallas_call(
        functools.partial(attention_kernel, n_sp, n_tp),
        out_shape=jax.ShapeDtypeStruct((n_tp, rows, cols), bf),
        in_specs=[hbm] * 4 + [vmem] * 4,
        out_specs=hbm,
        scratch_shapes=[
            pltpu.VMEM((n_sp, sub, HEAD), bf),
            pltpu.VMEM((n_sp, n_tp, 2, sub, HEAD), bf),
            pltpu.VMEM((n_sp, 8, HEAD), jnp.float32),
            pltpu.VMEM((n_sp, rows, HEAD), bf),
            pltpu.VMEM((n_sp, sub, HEAD), bf),
            pltpu.VMEM((n_tp, sub, width), bf),
            pltpu.VMEM((n_tp, rows, cols), bf),
            dma((2, n_tp, 4)),
            dma((n_sp + 2,)),
            dma((5,)),
            dma((4, n_sp)),
            dma((4,)),
            dma((5,)),
            dma((n_sp,)),
            dma,
            dma((2, 9)),
            dma((2, 9)),
            dma,
        ],
        compiler_params=pltpu.CompilerParams(
            collective_id=0, has_side_effects=True, vmem_limit_bytes=48 * 1024 * 1024
        ),
        cost_estimate=pl.CostEstimate(flops=40_000_000_000, bytes_accessed=100_000_000, transcendentals=0),
        name="attend",
    )(q, k, v, f, res, ow, qg.reshape(1, HEAD), kg.reshape(1, HEAD))
    ff = gw.shape[1]
    deep = n_tp * cols
    return pl.pallas_call(
        functools.partial(feed_forward_kernel, n_sp, n_tp),
        out_shape=jax.ShapeDtypeStruct((rows, cols), bf),
        in_specs=[hbm, hbm, vmem],
        out_specs=vmem,
        scratch_shapes=[
            pltpu.VMEM((n_tp, rows, cols), bf),
            pltpu.VMEM((ff, deep), bf),
            pltpu.VMEM((ff, deep), bf),
            pltpu.VMEM((ff, deep), bf),
            pltpu.VMEM((rows, deep), bf),
            pltpu.VMEM((rows, ff), bf),
            pltpu.VMEM((4, 2, rows, cols), bf),
            pltpu.VMEM((4, rows, cols), bf),
            pltpu.VMEM((3, rows, cols), bf),
            pltpu.VMEM((3, rows, cols), bf),
            dma((1 + 3 * n_sp,)),
            dma((4,)),
            dma((4,)),
            dma((3,)),
            dma((3,)),
        ],
        compiler_params=pltpu.CompilerParams(
            collective_id=1, has_side_effects=True, vmem_limit_bytes=48 * 1024 * 1024
        ),
        cost_estimate=pl.CostEstimate(flops=4_400_000_000, bytes_accessed=12_000_000, transcendentals=0),
        name="feed",
    )(mid, w, ng.reshape(n_tp, 1, cols))


def solution(mesh):
    whole = P(("grp", "sp"), "tp")
    weight = P("sp", "tp")
    placed = (whole,) * 5 + (P(), P(), P(None, "tp"), P(), weight, weight, weight)
    return jax.shard_map(
        functools.partial(local, mesh.shape["sp"], mesh.shape["tp"]),
        mesh=mesh,
        in_specs=placed,
        out_specs=whole,
        check_vma=False,
    )
```

```python
import functools
import math

import jax
import jax.numpy as jnp
from jax import lax
from jax.experimental import pallas as pl
from jax.experimental.pallas import tpu as pltpu
from jax.sharding import PartitionSpec as P

MESH = pl.DeviceIdType.MESH
HEAD = 128
EPS = 1e-06
LOW = -1e30
LOG2E = 1.4426950408889634


def remote(src, dst, send, recv, device):
    return pltpu.make_async_remote_copy(
        src_ref=src, dst_ref=dst, send_sem=send, recv_sem=recv, device_id=device, device_id_type=MESH
    )


def arrived(ref, sem, device):
    remote(ref, ref, sem, sem, device).wait_recv()


def left_over(ref, sem, device):
    remote(ref, ref, sem, sem, device).wait_send()


class Row:
    def __init__(self, t, size):
        self.t = t
        self.left = lax.rem(t + size - 2, size)
        self.right = lax.rem(t + 2, size)
        self.opp = lax.rem(t + size // 2, size)
        self.core = lax.rem(t, 2)

    @staticmethod
    def other(t):
        return t + 1 - 2 * lax.rem(t, 2)


def row_gather(row, buf, send, recv):
    half = buf.shape[1] // 2
    t, left, right, opp = row.t, row.left, row.right, row.opp
    other = Row.other
    to_left, to_right, to_other = {"tp": left}, {"tp": right}, {"tp": other(t)}
    first, second = pl.ds(0, half), pl.ds(half, half)
    sent = []

    def go(ref, at, device):
        copy = remote(ref, ref, send.at[at], recv.at[at], device)
        copy.start()
        sent.append(copy)

    go(buf.at[t], 0, to_right)
    go(buf.at[t], 1, to_left)
    go(buf.at[t], 2, to_other)
    arrived(buf.at[left], recv.at[0], to_left)
    go(buf.at[left, first], 3, to_right)
    go(buf.at[left], 4, to_other)
    arrived(buf.at[right], recv.at[1], to_right)
    go(buf.at[right, second], 5, to_left)
    go(buf.at[right], 6, to_other)
    arrived(buf.at[opp, first], recv.at[3], to_left)
    go(buf.at[opp, first], 7, to_other)
    arrived(buf.at[opp, second], recv.at[5], to_right)
    go(buf.at[opp, second], 8, to_other)
    arrived(buf.at[other(t)], recv.at[2], to_other)
    arrived(buf.at[other(left)], recv.at[4], to_other)
    arrived(buf.at[other(right)], recv.at[6], to_other)
    arrived(buf.at[other(opp), first], recv.at[7], to_other)
    arrived(buf.at[other(opp), second], recv.at[8], to_other)
    for copy in sent:
        copy.wait_send()


def normed(rows, gain):
    square = jnp.mean(rows * rows, axis=-1, keepdims=True)
    return rows * lax.rsqrt(square + EPS) * gain


def layer_kernel(
    n_sp,
    n_tp,
    q_ref,
    k_ref,
    v_ref,
    f_ref,
    res_ref,
    ow_ref,
    qg_ref,
    kg_ref,
    w_ref,
    gain_ref,
    out_ref,
    qbuf,
    kv,
    fbuf,
    kn,
    obuf,
    att,
    mid,
    send_a,
    recv_a,
    send_b,
    recv_b,
    send_c,
    recv_c,
    send_o,
    recv_o,
    send_g,
    recv_g,
    wbuf,
    nrm,
    hid,
    part,
    pair,
    total,
    landed,
    own_sem,
    send_w,
    recv_w,
    send_y,
    recv_y,
    send_p,
    recv_p,
    send_r,
    recv_r,
):
    s = lax.axis_index("sp")
    parity = lax.rem(lax.axis_index("grp"), 2)
    to_pair = {"grp": lax.axis_index("grp") + 1 - 2 * parity}
    to_next = {"sp": lax.rem(s + 1, n_sp)}
    to_last = {"sp": lax.rem(s + n_sp - 1, n_sp)}
    t = lax.axis_index("tp")
    row = Row(t, n_tp)
    other = Row.other
    left, right, opp = row.left, row.right, row.opp
    sub = qbuf.shape[1]
    per = n_sp // 4

    def row_of(head):
        return lax.rem(head, per) * 4 + head // per

    def head_of(r):
        return lax.rem(r, 4) * per + r // 4

    my_head = head_of(s)
    source = my_head // 2

    barrier = pltpu.get_barrier_semaphore()

    def hello(device):
        pl.semaphore_signal(barrier, inc=1, device_id=device, device_id_type=MESH)

    for peer in (left, right, opp, other(t)):
        hello({"tp": peer})
    hello(to_pair)

    @pl.loop(0, n_sp)
    def _(r):
        @pl.when(r != s)
        def _():
            hello({"sp": r, "tp": t})

        @pl.when(jnp.logical_or(r != s, t != source))
        def _():
            hello({"sp": r, "tp": source})

    own = jnp.logical_or(row_of(2 * t) == s, row_of(2 * t + 1) == s)
    pl.semaphore_wait(barrier, 5 + n_sp - 1 + 2 * n_tp - own.astype(jnp.int32))

    def pieces(u, hi, keys):
        there = lax.rem(t + u, n_tp)
        rows, cols = pl.ds(there * sub, sub), pl.ds(hi * HEAD, HEAD)
        if keys:
            return there, (
                (k_ref.at[rows, cols], kv.at[s, there, 0], 2, recv_a.at[s]),
                (v_ref.at[rows, cols], kv.at[s, there, 1], 3, recv_a.at[s]),
            )
        return there, (
            (q_ref.at[rows, cols], qbuf.at[s], 0, recv_a.at[n_sp]),
            (f_ref.at[hi], fbuf.at[s], 1, recv_a.at[n_sp + 1]),
        )

    def each_piece(act, start, keys):
        @pl.loop(0, n_tp)
        def _(u):
            for hi in range(2):
                r = row_of(2 * t + hi)
                there, list_of = pieces(u, hi, keys)
                mine = jnp.logical_and(r == s, there == t)

                @pl.when(jnp.logical_not(mine))
                def _():
                    for src, dst, i, sem in list_of:
                        act(remote(src, dst, send_a.at[hi, u, i], sem, {"sp": r, "tp": there}))

                if start:

                    @pl.when(mine)
                    def _():
                        for src, dst, _, sem in list_of:
                            pltpu.make_async_copy(src, dst, sem).start()

    third = w_ref.shape[0] // 3
    ringed = pl.ds(pl.multiple_of(parity * third, 16), 2 * third)
    shared = pl.ds(pl.multiple_of(parity * 2 * third, 16), third)
    half_way = n_sp // 2

    def chunk(d):
        return lax.rem(s + d + n_sp, n_sp)

    def pass_on(k, src, chunk_at, to, way):
        remote(src, wbuf.at[chunk_at, ringed], send_w.at[way, k], recv_w.at[way, k], to).start()

    def tick(k):
        here = chunk(-k)
        arrived(wbuf.at[here, ringed], recv_w.at[0, k - 1], to_last)

        @pl.when(k < half_way)
        def _():
            pass_on(k, wbuf.at[here, ringed], here, to_next, 0)

        piece = wbuf.at[here, shared]
        remote(piece, piece, send_y, recv_y, to_pair).start()

        @pl.when(k < half_way)
        def _():
            far = chunk(k)
            arrived(wbuf.at[far, ringed], recv_w.at[1, k - 1], to_next)

            @pl.when(k < half_way - 1)
            def _():
                pass_on(k, wbuf.at[far, ringed], far, to_last, 1)

            piece = wbuf.at[far, shared]
            remote(piece, piece, send_y, recv_y, to_pair).start()

    own_copy = pltpu.make_async_copy(w_ref, wbuf.at[s], own_sem)
    own_copy.start()
    each_piece(lambda c: c.start(), True, True)
    pass_on(0, w_ref.at[ringed], s, to_next, 0)
    pass_on(0, w_ref.at[ringed], s, to_last, 1)
    each_piece(lambda c: c.start(), True, False)

    to_left, to_right, to_other = {"tp": left}, {"tp": right}, {"tp": other(t)}

    def at_step(j):
        d = (j + 1) // 2
        return lax.rem(s + n_sp + jnp.where(lax.rem(j, 2) == 1, d, -d), n_sp)

    def stage_one(j):
        b = at_step(j)
        arrived(kv.at[b, t], recv_a.at[b], to_other)
        piece = kv.at[b, t]
        remote(piece, piece, send_b.at[0], recv_b.at[0, b], to_right).start()
        remote(piece, piece, send_b.at[1], recv_b.at[1, b], to_left).start()
        remote(piece, piece, send_b.at[2], recv_c.at[0], to_other).start()

    def stage_two(j):
        b = at_step(j)
        arrived(kv.at[b, left], recv_b.at[0, b], to_left)
        piece, part = kv.at[b, left], kv.at[b, left, 0]
        remote(part, part, send_b.at[3], recv_b.at[2, b], to_right).start()
        remote(piece, piece, send_c.at[0], recv_c.at[1], to_other).start()
        arrived(kv.at[b, right], recv_b.at[1, b], to_right)
        piece, part = kv.at[b, right], kv.at[b, right, 1]
        remote(part, part, send_b.at[4], recv_b.at[3, b], to_left).start()
        remote(piece, piece, send_c.at[1], recv_c.at[2], to_other).start()

    def stage_three(j):
        b = at_step(j)
        arrived(kv.at[b, opp, 0], recv_b.at[2, b], to_left)
        part = kv.at[b, opp, 0]
        remote(part, part, send_c.at[2], recv_c.at[3], to_other).start()
        arrived(kv.at[b, opp, 1], recv_b.at[3, b], to_right)
        part = kv.at[b, opp, 1]
        remote(part, part, send_c.at[3], recv_c.at[4], to_other).start()

    lag = 2

    @pl.loop(0, n_sp + 2 * lag)
    def _(j):
        @pl.when(j < n_sp)
        def _():
            stage_one(j)

        @pl.when(jnp.logical_and(j >= lag, j < n_sp + lag))
        def _():
            stage_two(j - lag)

        @pl.when(j >= 2 * lag)
        def _():
            stage_three(j - 2 * lag)

        @pl.when(lax.rem(j, 4) == 3)
        def _():
            tick(j // 4 + 1)

    arrived(kv.at[:, other(t)], recv_c.at[0], to_other)
    arrived(kv.at[:, other(left)], recv_c.at[1], to_other)
    arrived(kv.at[:, other(right)], recv_c.at[2], to_other)
    arrived(kv.at[:, other(opp), 0], recv_c.at[3], to_other)
    arrived(kv.at[:, other(opp), 1], recv_c.at[4], to_other)
    arrived(qbuf, recv_a.at[n_sp], to_other)
    arrived(fbuf, recv_a.at[n_sp + 1], to_other)

    width = n_tp * sub

    @pl.loop(0, n_sp)
    def _(b):
        rows = kv[b, :, 0].reshape(width, HEAD).astype(jnp.float32)
        kn[b] = normed(rows, kg_ref[...]).astype(jnp.bfloat16)

    group = 4
    tall, wide = group * sub, group * width
    factor = LOG2E / math.sqrt(HEAD)

    def bias_row(c, base):
        parts = []
        for b in range(group):
            slab = fbuf[c * group + b]
            for lane in range(width // HEAD):
                parts.append(slab[lane : lane + 1])
        return (base - jnp.concatenate(parts, axis=1)) * LOG2E

    @pl.loop(0, n_sp // group)
    def _(step):
        i = n_sp // group - 1 - step
        q = qbuf[pl.ds(i * group, group)].reshape(tall, HEAD).astype(jnp.float32)
        q = normed(q, qg_ref[...]).astype(jnp.bfloat16)
        base = fbuf[i * group, 0:1, 0:1]

        def visit(c, state, masked):
            top, total, acc = state
            keys = kn[pl.ds(c * group, group)].reshape(wide, HEAD)
            scores = lax.dot_general(q, keys, (((1,), (1,)), ((), ())), preferred_element_type=jnp.float32)
            scores = scores * factor + bias_row(c, base)
            if masked:
                line = lax.broadcasted_iota(jnp.int32, (tall, wide), 0)
                place = (line // sub) * width + t * sub + lax.rem(line, sub)
                scores = jnp.where(lax.broadcasted_iota(jnp.int32, (tall, wide), 1) <= place, scores, LOW)
            high = jnp.maximum(top, jnp.max(scores, axis=1, keepdims=True))
            raised = jnp.exp2(scores - high)
            shrink = jnp.exp2(top - high)
            total = total * shrink + jnp.sum(raised, axis=1, keepdims=True)
            vals = kv[pl.ds(c * group, group), :, 1].reshape(wide, HEAD)
            acc = acc * shrink + jnp.dot(raised.astype(jnp.bfloat16), vals, preferred_element_type=jnp.float32)
            return high, total, acc

        state = (
            jnp.full((tall, 1), LOW, jnp.float32),
            jnp.zeros((tall, 1), jnp.float32),
            jnp.zeros((tall, HEAD), jnp.float32),
        )
        state = visit(i, state, True)
        _, total, acc = lax.fori_loop(0, i, lambda c, st: visit(c, st, False), state)
        obuf[pl.ds(i * group, group)] = (acc / total).astype(jnp.bfloat16).reshape(group, sub, HEAD)

        @pl.loop(0, group)
        def _(n):
            r = i * group + n
            cols = pl.ds(pl.multiple_of(my_head * HEAD, HEAD), HEAD)

            @pl.when(r != s)
            def _():
                remote(obuf.at[r], att.at[t, :, cols], send_o.at[r], recv_o, {"sp": r, "tp": t}).start()

            @pl.when(r == s)
            def _():
                att[t, :, cols] = obuf[r]

    tick(6)

    def o_wait(r):
        @pl.when(r != s)
        def _():
            left_over(obuf.at[r], send_o.at[r], {"sp": r, "tp": t})

    pl.loop(0, n_sp)(o_wait)
    arrived(att.at[t, :, pl.ds(0, (n_sp - 1) * HEAD)], recv_o, to_other)

    tick(7)
    row_gather(row, att, send_g.at[0], recv_g.at[0])
    tick(8)
    total_rows = n_tp * sub
    span = 256

    @pl.loop(0, total_rows // span)
    def _(m):
        rows = pl.ds(m * span, span)
        lhs = att[pl.ds(m * (span // sub), span // sub)].reshape(span, att.shape[2])
        product = jnp.dot(lhs, ow_ref[...], preferred_element_type=jnp.float32)
        mid[t, rows] = (res_ref[rows].astype(jnp.float32) + product).astype(jnp.bfloat16)

    row_gather(row, mid, send_g.at[1], recv_g.at[1])
    cols = mid.shape[2]
    rows = mid.shape[1]
    core = row.core
    depth = wbuf.shape[2]
    span = 128

    @pl.loop(0, rows // span)
    def _(m):
        at = pl.ds(m * span, span)
        blocks = [mid[u, at].astype(jnp.float32) for u in range(n_tp)]
        square = sum(jnp.sum(b * b, axis=1, keepdims=True) for b in blocks) / (n_tp * cols)
        scale = lax.rsqrt(square + EPS)
        for u in range(n_tp):
            nrm[at, pl.ds(u * cols, cols)] = (blocks[u] * scale * gain_ref[u]).astype(jnp.bfloat16)

    own_copy.wait()
    arrived(wbuf.at[pl.ds(0, n_sp - 1), shared], recv_y, to_pair)

    def stacked(which, first, count):
        return jnp.concatenate([wbuf[first + z, pl.ds(which * third, third)] for z in range(count)], axis=1)

    tall = 256

    @pl.loop(0, rows // tall)
    def _(m):
        at = pl.ds(m * tall, tall)
        across = (((1,), (1,)), ((), ()))
        gate = lax.dot_general(nrm[at], stacked(0, 0, n_sp), across, preferred_element_type=jnp.float32)
        up = lax.dot_general(nrm[at], stacked(1, 0, n_sp), across, preferred_element_type=jnp.float32)
        hid[at] = (gate / (1.0 + jnp.exp(-gate)) * up).astype(jnp.bfloat16)

    chips = (opp, right, left, t)

    def add(k):
        arrived(pair.at[k], recv_p.at[k], to_other)
        mine = part[k, core].astype(jnp.float32) + pair[k].astype(jnp.float32)
        if k < 3:
            total[k] = mine.astype(jnp.bfloat16)
            remote(total.at[k], landed.at[k], send_r.at[k], recv_r.at[k], {"tp": chips[k]}).start()
            return None
        return mine

    for k in range(4):
        each = cols // depth
        for side in range(2):
            down = stacked(2, (chips[k] - core + side) * each, each)
            part[k, side] = jnp.dot(hid[...], down, preferred_element_type=jnp.float32).astype(jnp.bfloat16)
        remote(part.at[k, 1 - core], pair.at[k], send_p.at[k], recv_p.at[k], to_other).start()
        if k > 0:
            add(k - 1)
    mine = add(3) + mid[t].astype(jnp.float32)
    for k in (1, 2, 0):
        arrived(landed.at[k], recv_r.at[k], to_other)
        mine = mine + landed[k].astype(jnp.float32)
    out_ref[...] = mine.astype(jnp.bfloat16)
    for k in range(4):
        left_over(part.at[k, 1 - core], send_p.at[k], to_other)
    for k in range(3):
        left_over(total.at[k], send_r.at[k], {"tp": chips[k]})
    each_piece(lambda c: c.wait_send(), False, True)
    each_piece(lambda c: c.wait_send(), False, False)
    left_over(kv.at[:, t], send_b.at[0], to_right)
    left_over(kv.at[:, t], send_b.at[1], to_left)
    left_over(kv.at[:, t], send_b.at[2], to_other)
    left_over(kv.at[:, left, 0], send_b.at[3], to_right)
    left_over(kv.at[:, right, 1], send_b.at[4], to_left)
    left_over(kv.at[:, left], send_c.at[0], to_other)
    left_over(kv.at[:, right], send_c.at[1], to_other)
    left_over(kv.at[:, opp, 0], send_c.at[2], to_other)
    left_over(kv.at[:, opp, 1], send_c.at[3], to_other)
    for k in range(half_way):
        left_over(wbuf.at[s, ringed], send_w.at[0, k], to_next)
    for k in range(half_way - 1):
        left_over(wbuf.at[s, ringed], send_w.at[1, k], to_last)
    left_over(wbuf.at[pl.ds(0, n_sp - 1), shared], send_y, to_pair)


def local(n_sp, n_tp, q, k, v, f, res, qg, kg, ow, ng, gw, uw, dw):
    rows, cols = q.shape
    sub = rows // n_tp
    hbm = pl.BlockSpec(memory_space=pltpu.HBM)
    vmem = pl.BlockSpec(memory_space=pltpu.VMEM)
    dma = pltpu.SemaphoreType.DMA
    flat = jnp.concatenate((gw, uw, dw), axis=1).T
    f = jnp.pad(f.T.reshape(2, rows // HEAD, HEAD), ((0, 0), (0, 8 - rows // HEAD), (0, 0)))
    bf = jnp.bfloat16
    width = n_sp * HEAD
    ff = gw.shape[1]
    return pl.pallas_call(
        functools.partial(layer_kernel, n_sp, n_tp),
        out_shape=jax.ShapeDtypeStruct((rows, cols), bf),
        in_specs=[hbm] * 4 + [vmem] * 4 + [hbm, vmem],
        out_specs=vmem,
        scratch_shapes=[
            pltpu.VMEM((n_sp, sub, HEAD), bf),
            pltpu.VMEM((n_sp, n_tp, 2, sub, HEAD), bf),
            pltpu.VMEM((n_sp, 8, HEAD), jnp.float32),
            pltpu.VMEM((n_sp, rows, HEAD), bf),
            pltpu.VMEM((n_sp, sub, HEAD), bf),
            pltpu.VMEM((n_tp, sub, width), bf),
            pltpu.VMEM((n_tp, rows, cols), bf),
            dma((2, n_tp, 4)),
            dma((n_sp + 2,)),
            dma((5,)),
            dma((4, n_sp)),
            dma((4,)),
            dma((5,)),
            dma((n_sp,)),
            dma,
            dma((2, 9)),
            dma((2, 9)),
            pltpu.VMEM((n_sp, 3 * ff, gw.shape[0]), bf),
            pltpu.VMEM((rows, n_tp * cols), bf),
            pltpu.VMEM((rows, ff), bf),
            pltpu.VMEM((4, 2, rows, cols), bf),
            pltpu.VMEM((4, rows, cols), bf),
            pltpu.VMEM((3, rows, cols), bf),
            pltpu.VMEM((3, rows, cols), bf),
            dma,
            dma((2, n_sp // 2)),
            dma((2, n_sp // 2)),
            dma,
            dma,
            dma((4,)),
            dma((4,)),
            dma((3,)),
            dma((3,)),
        ],
        compiler_params=pltpu.CompilerParams(
            collective_id=0, has_side_effects=True, vmem_limit_bytes=60 * 1024 * 1024
        ),
        cost_estimate=pl.CostEstimate(flops=40_000_000_000, bytes_accessed=100_000_000, transcendentals=0),
        name="layer",
    )(q, k, v, f, res, ow, qg.reshape(1, HEAD), kg.reshape(1, HEAD), flat, ng.reshape(n_tp, 1, cols))


def solution(mesh):
    whole = P(("grp", "sp"), "tp")
    weight = P("sp", "tp")
    placed = (whole,) * 5 + (P(), P(), P(None, "tp"), P(), weight, weight, weight)
    return jax.shard_map(
        functools.partial(local, mesh.shape["sp"], mesh.shape["tp"]),
        mesh=mesh,
        in_specs=placed,
        out_specs=whole,
        check_vma=False,
    )
```

```python
import functools
import math

import jax
import jax.numpy as jnp
from jax import lax
from jax.experimental import pallas as pl
from jax.experimental.pallas import tpu as pltpu
from jax.sharding import PartitionSpec as P

MESH = pl.DeviceIdType.MESH
HEAD = 128
EPS = 1e-06
LOW = -1e30
LOG2E = 1.4426950408889634


def remote(src, dst, send, recv, device):
    return pltpu.make_async_remote_copy(
        src_ref=src, dst_ref=dst, send_sem=send, recv_sem=recv, device_id=device, device_id_type=MESH
    )


def arrived(ref, sem, device):
    remote(ref, ref, sem, sem, device).wait_recv()


def left_over(ref, sem, device):
    remote(ref, ref, sem, sem, device).wait_send()


class Row:
    def __init__(self, t, size):
        self.t = t
        self.left = lax.rem(t + size - 2, size)
        self.right = lax.rem(t + 2, size)
        self.opp = lax.rem(t + size // 2, size)
        self.core = lax.rem(t, 2)

    @staticmethod
    def other(t):
        return t + 1 - 2 * lax.rem(t, 2)


def row_gather(row, buf, send, recv, between=lambda: None):
    half = buf.shape[1] // 2
    t, left, right, opp = row.t, row.left, row.right, row.opp
    other = Row.other
    to_left, to_right, to_other = {"tp": left}, {"tp": right}, {"tp": other(t)}
    first, second = pl.ds(0, half), pl.ds(half, half)
    sent = []

    def go(ref, at, device):
        copy = remote(ref, ref, send.at[at], recv.at[at], device)
        copy.start()
        sent.append(copy)

    go(buf.at[t], 0, to_right)
    go(buf.at[t], 1, to_left)
    go(buf.at[t], 2, to_other)
    arrived(buf.at[left], recv.at[0], to_left)
    go(buf.at[left, first], 3, to_right)
    go(buf.at[left], 4, to_other)
    arrived(buf.at[right], recv.at[1], to_right)
    go(buf.at[right, second], 5, to_left)
    go(buf.at[right], 6, to_other)
    arrived(buf.at[opp, first], recv.at[3], to_left)
    go(buf.at[opp, first], 7, to_other)
    arrived(buf.at[opp, second], recv.at[5], to_right)
    go(buf.at[opp, second], 8, to_other)
    between()
    arrived(buf.at[other(t)], recv.at[2], to_other)
    arrived(buf.at[other(left)], recv.at[4], to_other)
    arrived(buf.at[other(right)], recv.at[6], to_other)
    arrived(buf.at[other(opp), first], recv.at[7], to_other)
    arrived(buf.at[other(opp), second], recv.at[8], to_other)
    for copy in sent:
        copy.wait_send()


def normed(rows, gain):
    square = jnp.mean(rows * rows, axis=-1, keepdims=True)
    return rows * lax.rsqrt(square + EPS) * gain


def layer_kernel(
    n_sp,
    n_tp,
    q_ref,
    k_ref,
    v_ref,
    f_ref,
    res_ref,
    ow_ref,
    qg_ref,
    kg_ref,
    w_ref,
    gain_ref,
    out_ref,
    qbuf,
    kv,
    fbuf,
    kn,
    obuf,
    att,
    mid,
    send_a,
    recv_a,
    send_b,
    recv_b,
    send_c,
    recv_c,
    send_o,
    recv_o,
    send_g,
    recv_g,
    wbuf,
    nrm,
    hid,
    part,
    pair,
    total,
    landed,
    xbuf,
    xf,
    send_x,
    recv_x,
    send_d,
    own_sem,
    send_w,
    recv_w,
    send_y,
    recv_y,
    send_p,
    recv_p,
    send_r,
    recv_r,
):
    s = lax.axis_index("sp")
    parity = lax.rem(lax.axis_index("grp"), 2)
    to_pair = {"grp": lax.axis_index("grp") + 1 - 2 * parity}
    to_next = {"sp": lax.rem(s + 1, n_sp)}
    to_last = {"sp": lax.rem(s + n_sp - 1, n_sp)}
    t = lax.axis_index("tp")
    row = Row(t, n_tp)
    other = Row.other
    left, right, opp = row.left, row.right, row.opp
    sub = qbuf.shape[1]
    per = n_sp // 4

    def row_of(head):
        return lax.rem(head, per) * 4 + head // per

    def head_of(r):
        return lax.rem(r, 4) * per + r // 4

    my_head = head_of(s)
    source = my_head // 2

    barrier = pltpu.get_barrier_semaphore()

    def hello(device):
        pl.semaphore_signal(barrier, inc=1, device_id=device, device_id_type=MESH)

    hello(to_pair)

    @pl.loop(0, n_sp)
    def _(r):
        @pl.when(r != s)
        def _():
            hello({"sp": r})

    @pl.loop(0, n_tp)
    def _(peer):
        @pl.when(peer != t)
        def _():
            hello({"tp": peer})

    pl.semaphore_wait(barrier, n_sp + n_tp - 1)
    own = t == source
    whole = pl.ds(0, sub)

    def scatter(which):
        @pl.loop(0, n_tp)
        def _(i):
            there = lax.rem(t - s - i + n_sp + n_tp, n_tp)
            rows = pl.ds(there * sub, sub)
            cols = pl.ds(pl.multiple_of(lax.rem(my_head, 2) * HEAD, HEAD), HEAD)
            for at in which:
                ref = (k_ref, v_ref, q_ref)[at]
                sem = recv_x.at[t, at]

                @pl.when(there != t)
                def _():
                    remote(ref.at[rows], xbuf.at[t, at], send_x.at[at], sem, {"tp": there}).start()

                @pl.when(there == t)
                def _():
                    pltpu.make_async_copy(ref.at[rows], xbuf.at[t, at], sem).start()

                place = (kv.at[s, there, 0], kv.at[s, there, 1], qbuf.at[s])[at]
                sem_a = recv_a.at[n_sp] if at == 2 else recv_a.at[s]

                @pl.when(jnp.logical_and(own, there != t))
                def _():
                    remote(ref.at[rows, cols], place, send_d.at[at], sem_a, {"tp": there}).start()

                @pl.when(jnp.logical_and(own, there == t))
                def _():
                    pltpu.make_async_copy(ref.at[rows, cols], place, sem_a).start()

            if 2 in which:
                mine = f_ref.at[lax.rem(my_head, 2)]

                @pl.when(there != t)
                def _():
                    remote(f_ref, xf.at[t], send_x.at[3], recv_x.at[t, 3], {"tp": there}).start()

                @pl.when(there == t)
                def _():
                    pltpu.make_async_copy(f_ref, xf.at[t], recv_x.at[t, 3]).start()

                @pl.when(jnp.logical_and(own, there != t))
                def _():
                    remote(mine, fbuf.at[s], send_d.at[3], recv_a.at[n_sp + 1], {"tp": there}).start()

                @pl.when(jnp.logical_and(own, there == t))
                def _():
                    pltpu.make_async_copy(mine, fbuf.at[s], recv_a.at[n_sp + 1]).start()

    def deliver(which):
        @pl.loop(0, n_tp)
        def _(i):
            src = lax.rem(t + s + i, n_tp)
            if 2 in which:
                arrived(xbuf.at[src, 2], recv_x.at[src, 2], {"tp": other(t)})
                arrived(xf.at[src], recv_x.at[src, 3], {"tp": other(t)})
            else:
                arrived(xbuf.at[src, 0], recv_x.at[src, 0], {"tp": other(t)})
                arrived(xbuf.at[src, 1], recv_x.at[src, 1], {"tp": other(t)})
            for hi in range(2):
                r = row_of(2 * src + hi)
                cols = pl.ds(hi * HEAD, HEAD)

                @pl.when(r != s)
                def _():
                    for at in which:
                        place = (kv.at[s, t, 0], kv.at[s, t, 1], qbuf.at[s])[at]
                        sem_a = recv_a.at[n_sp] if at == 2 else recv_a.at[s]
                        remote(xbuf.at[src, at, whole, cols], place, send_a.at[at], sem_a, {"sp": r}).start()
                    if 2 in which:
                        remote(xf.at[src, hi], fbuf.at[s], send_a.at[3], recv_a.at[n_sp + 1], {"sp": r}).start()

    third = w_ref.shape[0] // 3
    on_ring = w_ref.shape[0] // 32 * 16 + 16
    ringed = pl.ds(pl.multiple_of(parity * (3 * third - on_ring), 16), on_ring)
    shared = pl.ds(pl.multiple_of(parity * on_ring, 16), 3 * third - on_ring)
    half_way = n_sp // 2

    def chunk(d):
        return lax.rem(s + d + n_sp, n_sp)

    def pass_on(k, src, chunk_at, to, way):
        remote(src, wbuf.at[chunk_at, ringed], send_w.at[way, k], recv_w.at[way, k], to).start()

    def tick(k):
        here = chunk(-k)
        arrived(wbuf.at[here, ringed], recv_w.at[0, k - 1], to_last)

        @pl.when(k < half_way)
        def _():
            pass_on(k, wbuf.at[here, ringed], here, to_next, 0)

        piece = wbuf.at[here, shared]
        remote(piece, piece, send_y, recv_y, to_pair).start()

        @pl.when(k < half_way)
        def _():
            far = chunk(k)
            arrived(wbuf.at[far, ringed], recv_w.at[1, k - 1], to_next)

            @pl.when(k < half_way - 1)
            def _():
                pass_on(k, wbuf.at[far, ringed], far, to_last, 1)

            piece = wbuf.at[far, shared]
            remote(piece, piece, send_y, recv_y, to_pair).start()

    own_copy = pltpu.make_async_copy(w_ref, wbuf.at[s], own_sem)
    own_copy.start()
    scatter((0, 1))
    scatter((2,))
    deliver((0, 1))
    deliver((2,))

    to_left, to_right, to_other = {"tp": left}, {"tp": right}, {"tp": other(t)}

    per_turn = n_sp // n_tp

    def at_step(owner, j):
        return lax.rem(source - owner - j // per_turn + 2 * n_tp, n_tp) + n_tp * lax.rem(j, per_turn)

    def stage_one(j):
        b = at_step(t, j)
        arrived(kv.at[b, t], recv_a.at[b], to_other)
        piece = kv.at[b, t]
        remote(piece, piece, send_b.at[0], recv_b.at[0, b], to_right).start()
        remote(piece, piece, send_b.at[1], recv_b.at[1, b], to_left).start()
        remote(piece, piece, send_b.at[2], recv_c.at[0], to_other).start()

    def stage_two(j):
        b = at_step(left, j)
        arrived(kv.at[b, left], recv_b.at[0, b], to_left)
        piece, half = kv.at[b, left], kv.at[b, left, 0]
        remote(half, half, send_b.at[3], recv_b.at[2, b], to_right).start()
        remote(piece, piece, send_c.at[0], recv_c.at[1], to_other).start()
        b = at_step(right, j)
        arrived(kv.at[b, right], recv_b.at[1, b], to_right)
        piece, half = kv.at[b, right], kv.at[b, right, 1]
        remote(half, half, send_b.at[4], recv_b.at[3, b], to_left).start()
        remote(piece, piece, send_c.at[1], recv_c.at[2], to_other).start()

    def stage_three(j):
        b = at_step(opp, j)
        for i, (way, device) in enumerate(((2, to_left), (3, to_right))):
            half = kv.at[b, opp, i]
            arrived(half, recv_b.at[way, b], device)
            remote(half, half, send_c.at[2 + i], recv_c.at[3 + i], to_other).start()

    lag = 2

    @pl.loop(0, n_sp + 2 * lag)
    def _(j):
        @pl.when(j < n_sp)
        def _():
            stage_one(j)

        @pl.when(jnp.logical_and(j >= lag, j < n_sp + lag))
        def _():
            stage_two(j - lag)

        @pl.when(j >= 2 * lag)
        def _():
            stage_three(j - 2 * lag)

        @pl.when(lax.rem(j, 8) == 0)
        def _():
            @pl.when(j == 0)
            def _():
                pass_on(0, w_ref.at[ringed], s, to_next, 0)
                pass_on(0, w_ref.at[ringed], s, to_last, 1)

            @pl.when(j > 0)
            def _():
                tick(j // 8)

    arrived(kv.at[:, other(t)], recv_c.at[0], to_other)
    arrived(kv.at[:, other(left)], recv_c.at[1], to_other)
    arrived(kv.at[:, other(right)], recv_c.at[2], to_other)
    arrived(kv.at[:, other(opp), 0], recv_c.at[3], to_other)
    arrived(kv.at[:, other(opp), 1], recv_c.at[4], to_other)
    arrived(qbuf, recv_a.at[n_sp], to_other)
    arrived(fbuf, recv_a.at[n_sp + 1], to_other)

    width = n_tp * sub

    @pl.loop(0, n_sp)
    def _(b):
        rows = kv[b, :, 0].reshape(width, HEAD).astype(jnp.float32)
        kn[b] = normed(rows, kg_ref[...]).astype(jnp.bfloat16)

    tick(3)
    group = 4
    tall, wide = group * sub, group * width
    factor = LOG2E / math.sqrt(HEAD)

    def bias_row(c, base):
        parts = []
        for b in range(group):
            slab = fbuf[c * group + b]
            for lane in range(width // HEAD):
                parts.append(slab[lane : lane + 1])
        return (base - jnp.concatenate(parts, axis=1)) * LOG2E

    @pl.loop(0, n_sp // group)
    def _(step):
        i = lax.rem(s + step, n_sp // group)

        @pl.when(step == 2)
        def _():
            tick(4)

        q = qbuf[pl.ds(i * group, group)].reshape(tall, HEAD).astype(jnp.float32)
        q = normed(q, qg_ref[...]).astype(jnp.bfloat16)
        base = fbuf[i * group, 0:1, 0:1]

        def visit(c, state, masked):
            top, total, acc = state
            keys = kn[pl.ds(c * group, group)].reshape(wide, HEAD)
            scores = lax.dot_general(q, keys, (((1,), (1,)), ((), ())), preferred_element_type=jnp.float32)
            scores = scores * factor + bias_row(c, base)
            if masked:
                line = lax.broadcasted_iota(jnp.int32, (tall, wide), 0)
                place = (line // sub) * width + t * sub + lax.rem(line, sub)
                scores = jnp.where(lax.broadcasted_iota(jnp.int32, (tall, wide), 1) <= place, scores, LOW)
            high = jnp.maximum(top, jnp.max(scores, axis=1, keepdims=True))
            raised = jnp.exp2(scores - high)
            shrink = jnp.exp2(top - high)
            total = total * shrink + jnp.sum(raised, axis=1, keepdims=True)
            vals = kv[pl.ds(c * group, group), :, 1].reshape(wide, HEAD)
            acc = acc * shrink + jnp.dot(raised.astype(jnp.bfloat16), vals, preferred_element_type=jnp.float32)
            return high, total, acc

        state = (
            jnp.full((tall, 1), LOW, jnp.float32),
            jnp.zeros((tall, 1), jnp.float32),
            jnp.zeros((tall, HEAD), jnp.float32),
        )
        state = visit(i, state, True)
        _, total, acc = lax.fori_loop(0, i, lambda c, st: visit(c, st, False), state)
        obuf[pl.ds(i * group, group)] = (acc / total).astype(jnp.bfloat16).reshape(group, sub, HEAD)

        @pl.loop(0, group)
        def _(n):
            r = i * group + n
            cols = pl.ds(pl.multiple_of(my_head * HEAD, HEAD), HEAD)

            @pl.when(r != s)
            def _():
                remote(obuf.at[r], att.at[t, :, cols], send_o.at[r], recv_o, {"sp": r, "tp": t}).start()

            @pl.when(r == s)
            def _():
                att[t, :, cols] = obuf[r]

    tick(5)

    def o_wait(r):
        @pl.when(r != s)
        def _():
            left_over(obuf.at[r], send_o.at[r], {"sp": r, "tp": t})

    pl.loop(0, n_sp)(o_wait)
    tick(6)
    arrived(att.at[t, :, pl.ds(0, (n_sp - 1) * HEAD)], recv_o, to_other)

    row_gather(row, att, send_g.at[0], recv_g.at[0], lambda: tick(7))
    tick(8)
    total_rows = n_tp * sub
    span = 256

    @pl.loop(0, total_rows // span)
    def _(m):
        rows = pl.ds(m * span, span)
        lhs = att[pl.ds(m * (span // sub), span // sub)].reshape(span, att.shape[2])
        product = jnp.dot(lhs, ow_ref[...], preferred_element_type=jnp.float32)
        mid[t, rows] = (res_ref[rows].astype(jnp.float32) + product).astype(jnp.bfloat16)

    row_gather(row, mid, send_g.at[1], recv_g.at[1])
    cols = mid.shape[2]
    rows = mid.shape[1]
    core = row.core
    depth = wbuf.shape[2]
    span = 128

    @pl.loop(0, rows // span)
    def _(m):
        at = pl.ds(m * span, span)
        blocks = [mid[u, at].astype(jnp.float32) for u in range(n_tp)]
        square = sum(jnp.sum(b * b, axis=1, keepdims=True) for b in blocks) / (n_tp * cols)
        scale = lax.rsqrt(square + EPS)
        for u in range(n_tp):
            nrm[at, pl.ds(u * cols, cols)] = (blocks[u] * scale * gain_ref[u]).astype(jnp.bfloat16)

    own_copy.wait()
    arrived(wbuf.at[pl.ds(0, n_sp - 1), shared], recv_y, to_pair)

    def stacked(which, first, count):
        return jnp.concatenate([wbuf[first + z, pl.ds(which * third, third)] for z in range(count)], axis=1)

    tall = 256

    @pl.loop(0, rows // tall)
    def _(m):
        at = pl.ds(m * tall, tall)
        across = (((1,), (1,)), ((), ()))
        gate = lax.dot_general(nrm[at], stacked(0, 0, n_sp), across, preferred_element_type=jnp.float32)
        up = lax.dot_general(nrm[at], stacked(1, 0, n_sp), across, preferred_element_type=jnp.float32)
        hid[at] = (gate / (1.0 + jnp.exp(-gate)) * up).astype(jnp.bfloat16)

    chips = (opp, right, left, t)

    def add(k):
        arrived(pair.at[k], recv_p.at[k], to_other)
        mine = part[k, core].astype(jnp.float32) + pair[k].astype(jnp.float32)
        if k < 3:
            total[k] = mine.astype(jnp.bfloat16)
            remote(total.at[k], landed.at[k], send_r.at[k], recv_r.at[k], {"tp": chips[k]}).start()
            return None
        return mine

    for k in range(4):
        each = cols // depth
        for side in range(2):
            down = stacked(2, (chips[k] - core + side) * each, each)
            part[k, side] = jnp.dot(hid[...], down, preferred_element_type=jnp.float32).astype(jnp.bfloat16)
        remote(part.at[k, 1 - core], pair.at[k], send_p.at[k], recv_p.at[k], to_other).start()
        if k > 0:
            add(k - 1)
    mine = add(3) + mid[t].astype(jnp.float32)
    for k in (1, 2, 0):
        arrived(landed.at[k], recv_r.at[k], to_other)
        mine = mine + landed[k].astype(jnp.float32)
    out_ref[...] = mine.astype(jnp.bfloat16)
    for k in range(4):
        left_over(part.at[k, 1 - core], send_p.at[k], to_other)
    for k in range(3):
        left_over(total.at[k], send_r.at[k], {"tp": chips[k]})
    for at, ref in enumerate((k_ref, v_ref, q_ref)):
        left_over(ref.at[pl.ds(0, (n_tp - 1) * sub)], send_x.at[at], to_other)
        left_over(qbuf.at[pl.ds(0, n_sp - 1)], send_a.at[at], to_other)
    left_over(xf.at[pl.ds(0, n_tp - 1)], send_x.at[3], to_other)
    left_over(fbuf.at[pl.ds(0, n_sp - 1)], send_a.at[3], to_other)

    @pl.when(own)
    def _():
        for at in range(3):
            left_over(qbuf.at[pl.ds(0, n_tp - 1)], send_d.at[at], to_other)
        left_over(fbuf.at[pl.ds(0, n_tp - 1)], send_d.at[3], to_other)

    left_over(kv.at[:, t], send_b.at[0], to_right)
    left_over(kv.at[:, t], send_b.at[1], to_left)
    left_over(kv.at[:, t], send_b.at[2], to_other)
    left_over(kv.at[:, left, 0], send_b.at[3], to_right)
    left_over(kv.at[:, right, 1], send_b.at[4], to_left)
    left_over(kv.at[:, left], send_c.at[0], to_other)
    left_over(kv.at[:, right], send_c.at[1], to_other)
    left_over(kv.at[:, opp, 0], send_c.at[2], to_other)
    left_over(kv.at[:, opp, 1], send_c.at[3], to_other)
    for k in range(half_way):
        left_over(wbuf.at[s, ringed], send_w.at[0, k], to_next)
    for k in range(half_way - 1):
        left_over(wbuf.at[s, ringed], send_w.at[1, k], to_last)
    left_over(wbuf.at[pl.ds(0, n_sp - 1), shared], send_y, to_pair)


def local(n_sp, n_tp, q, k, v, f, res, qg, kg, ow, ng, gw, uw, dw):
    rows, cols = q.shape
    sub = rows // n_tp
    hbm = pl.BlockSpec(memory_space=pltpu.HBM)
    vmem = pl.BlockSpec(memory_space=pltpu.VMEM)
    dma = pltpu.SemaphoreType.DMA
    flat = jnp.concatenate((gw, uw, dw), axis=1).T
    f = jnp.pad(f.T.reshape(2, rows // HEAD, HEAD), ((0, 0), (0, 8 - rows // HEAD), (0, 0)))
    bf = jnp.bfloat16
    width = n_sp * HEAD
    ff = gw.shape[1]
    return pl.pallas_call(
        functools.partial(layer_kernel, n_sp, n_tp),
        out_shape=jax.ShapeDtypeStruct((rows, cols), bf),
        in_specs=[hbm] * 4 + [vmem] * 4 + [hbm, vmem],
        out_specs=vmem,
        scratch_shapes=[
            pltpu.VMEM((n_sp, sub, HEAD), bf),
            pltpu.VMEM((n_sp, n_tp, 2, sub, HEAD), bf),
            pltpu.VMEM((n_sp, 8, HEAD), jnp.float32),
            pltpu.VMEM((n_sp, rows, HEAD), bf),
            pltpu.VMEM((n_sp, sub, HEAD), bf),
            pltpu.VMEM((n_tp, sub, width), bf),
            pltpu.VMEM((n_tp, rows, cols), bf),
            dma((4,)),
            dma((n_sp + 2,)),
            dma((5,)),
            dma((4, n_sp)),
            dma((4,)),
            dma((5,)),
            dma((n_sp,)),
            dma,
            dma((2, 9)),
            dma((2, 9)),
            pltpu.VMEM((n_sp, 3 * ff, gw.shape[0]), bf),
            pltpu.VMEM((rows, n_tp * cols), bf),
            pltpu.VMEM((rows, ff), bf),
            pltpu.VMEM((4, 2, rows, cols), bf),
            pltpu.VMEM((4, rows, cols), bf),
            pltpu.VMEM((3, rows, cols), bf),
            pltpu.VMEM((3, rows, cols), bf),
            pltpu.VMEM((n_tp, 3, sub, cols), bf),
            pltpu.VMEM((n_tp, 2, 8, HEAD), jnp.float32),
            dma((4,)),
            dma((n_tp, 4)),
            dma((4,)),
            dma,
            dma((2, n_sp // 2)),
            dma((2, n_sp // 2)),
            dma,
            dma,
            dma((4,)),
            dma((4,)),
            dma((3,)),
            dma((3,)),
        ],
        compiler_params=pltpu.CompilerParams(
            collective_id=0, has_side_effects=True, vmem_limit_bytes=60 * 1024 * 1024
        ),
        cost_estimate=pl.CostEstimate(flops=40_000_000_000, bytes_accessed=100_000_000, transcendentals=0),
        name="layer",
    )(q, k, v, f, res, ow, qg.reshape(1, HEAD), kg.reshape(1, HEAD), flat, ng.reshape(n_tp, 1, cols))


def solution(mesh):
    whole = P(("grp", "sp"), "tp")
    weight = P("sp", "tp")
    placed = (whole,) * 5 + (P(), P(), P(None, "tp"), P(), weight, weight, weight)
    return jax.shard_map(
        functools.partial(local, mesh.shape["sp"], mesh.shape["tp"]),
        mesh=mesh,
        in_specs=placed,
        out_specs=whole,
        check_vma=False,
    )
```

```python
import functools
import math

import jax
import jax.numpy as jnp
from jax import lax
from jax.experimental import pallas as pl
from jax.experimental.pallas import tpu as pltpu
from jax.sharding import PartitionSpec as P

MESH = pl.DeviceIdType.MESH
HEAD = 128
EPS = 1e-06
LOW = -1e30
LOG2E = 1.4426950408889634


def remote(src, dst, send, recv, device):
    return pltpu.make_async_remote_copy(
        src_ref=src, dst_ref=dst, send_sem=send, recv_sem=recv, device_id=device, device_id_type=MESH
    )


def arrived(ref, sem, device):
    remote(ref, ref, sem, sem, device).wait_recv()


def left_over(ref, sem, device):
    remote(ref, ref, sem, sem, device).wait_send()


class Row:
    def __init__(self, t, size):
        self.t = t
        self.left = lax.rem(t + size - 2, size)
        self.right = lax.rem(t + 2, size)
        self.opp = lax.rem(t + size // 2, size)
        self.core = lax.rem(t, 2)

    @staticmethod
    def other(t):
        return t + 1 - 2 * lax.rem(t, 2)


def row_gather(row, buf, send, recv, between=lambda: None):
    half = buf.shape[1] // 2
    t, left, right, opp = row.t, row.left, row.right, row.opp
    other = Row.other
    to_left, to_right, to_other = {"tp": left}, {"tp": right}, {"tp": other(t)}
    first, second = pl.ds(0, half), pl.ds(half, half)
    sent = []

    def go(ref, at, device):
        copy = remote(ref, ref, send.at[at], recv.at[at], device)
        copy.start()
        sent.append(copy)

    go(buf.at[t], 0, to_right)
    go(buf.at[t], 1, to_left)
    go(buf.at[t], 2, to_other)
    arrived(buf.at[left], recv.at[0], to_left)
    go(buf.at[left, first], 3, to_right)
    go(buf.at[left], 4, to_other)
    arrived(buf.at[right], recv.at[1], to_right)
    go(buf.at[right, second], 5, to_left)
    go(buf.at[right], 6, to_other)
    arrived(buf.at[opp, first], recv.at[3], to_left)
    go(buf.at[opp, first], 7, to_other)
    arrived(buf.at[opp, second], recv.at[5], to_right)
    go(buf.at[opp, second], 8, to_other)
    between()
    arrived(buf.at[other(t)], recv.at[2], to_other)
    arrived(buf.at[other(left)], recv.at[4], to_other)
    arrived(buf.at[other(right)], recv.at[6], to_other)
    arrived(buf.at[other(opp), first], recv.at[7], to_other)
    arrived(buf.at[other(opp), second], recv.at[8], to_other)
    for copy in sent:
        copy.wait_send()


def normed(rows, gain):
    square = jnp.mean(rows * rows, axis=-1, keepdims=True)
    return rows * lax.rsqrt(square + EPS) * gain


def layer_kernel(
    n_sp,
    n_tp,
    q_ref,
    k_ref,
    v_ref,
    f_ref,
    res_ref,
    ow_ref,
    qg_ref,
    kg_ref,
    w_ref,
    gain_ref,
    out_ref,
    qbuf,
    kv,
    fbuf,
    kn,
    obuf,
    att,
    mid,
    send_a,
    recv_a,
    send_b,
    recv_b,
    send_c,
    recv_c,
    send_o,
    recv_o,
    send_g,
    recv_g,
    wbuf,
    nrm,
    hid,
    part,
    pair,
    total,
    landed,
    xbuf,
    xf,
    send_x,
    recv_x,
    send_d,
    own_sem,
    send_w,
    recv_w,
    send_y,
    recv_y,
    send_p,
    recv_p,
    send_r,
    recv_r,
):
    s = lax.axis_index("sp")
    parity = lax.rem(lax.axis_index("grp"), 2)
    to_pair = {"grp": lax.axis_index("grp") + 1 - 2 * parity}
    to_next = {"sp": lax.rem(s + 1, n_sp)}
    to_last = {"sp": lax.rem(s + n_sp - 1, n_sp)}
    t = lax.axis_index("tp")
    row = Row(t, n_tp)
    other = Row.other
    left, right, opp = row.left, row.right, row.opp
    sub = qbuf.shape[1]
    per = n_sp // 4

    def row_of(head):
        return lax.rem(head, per) * 4 + head // per

    def head_of(r):
        return lax.rem(r, 4) * per + r // 4

    my_head = head_of(s)
    source = my_head // 2

    barrier = pltpu.get_barrier_semaphore()

    def hello(device):
        pl.semaphore_signal(barrier, inc=1, device_id=device, device_id_type=MESH)

    hello(to_pair)

    @pl.loop(0, n_sp)
    def _(r):
        @pl.when(r != s)
        def _():
            hello({"sp": r})

    @pl.loop(0, n_tp)
    def _(peer):
        @pl.when(peer != t)
        def _():
            hello({"tp": peer})

    pl.semaphore_wait(barrier, n_sp + n_tp - 1)
    own = t == source
    whole = pl.ds(0, sub)

    def scatter(which):
        @pl.loop(0, n_tp)
        def _(i):
            there = lax.rem(t - s - i + n_sp + n_tp, n_tp)
            rows = pl.ds(there * sub, sub)
            cols = pl.ds(pl.multiple_of(lax.rem(my_head, 2) * HEAD, HEAD), HEAD)
            for at in which:
                ref = (k_ref, v_ref, q_ref)[at]
                sem = recv_x.at[t, at]

                @pl.when(there != t)
                def _():
                    remote(ref.at[rows], xbuf.at[t, at], send_x.at[at], sem, {"tp": there}).start()

                @pl.when(there == t)
                def _():
                    pltpu.make_async_copy(ref.at[rows], xbuf.at[t, at], sem).start()

                place = (kv.at[s, there, 0], kv.at[s, there, 1], qbuf.at[s])[at]
                sem_a = recv_a.at[n_sp] if at == 2 else recv_a.at[s]

                @pl.when(jnp.logical_and(own, there != t))
                def _():
                    remote(ref.at[rows, cols], place, send_d.at[at], sem_a, {"tp": there}).start()

                @pl.when(jnp.logical_and(own, there == t))
                def _():
                    pltpu.make_async_copy(ref.at[rows, cols], place, sem_a).start()

            if 2 in which:
                mine = f_ref.at[lax.rem(my_head, 2)]

                @pl.when(there != t)
                def _():
                    remote(f_ref, xf.at[t], send_x.at[3], recv_x.at[t, 3], {"tp": there}).start()

                @pl.when(there == t)
                def _():
                    pltpu.make_async_copy(f_ref, xf.at[t], recv_x.at[t, 3]).start()

                @pl.when(jnp.logical_and(own, there != t))
                def _():
                    remote(mine, fbuf.at[s], send_d.at[3], recv_a.at[n_sp + 1], {"tp": there}).start()

                @pl.when(jnp.logical_and(own, there == t))
                def _():
                    pltpu.make_async_copy(mine, fbuf.at[s], recv_a.at[n_sp + 1]).start()

    def deliver(which):
        @pl.loop(0, n_tp)
        def _(i):
            src = lax.rem(t + s + i, n_tp)
            if 2 in which:
                arrived(xbuf.at[src, 2], recv_x.at[src, 2], {"tp": other(t)})
                arrived(xf.at[src], recv_x.at[src, 3], {"tp": other(t)})
            else:
                arrived(xbuf.at[src, 0], recv_x.at[src, 0], {"tp": other(t)})
                arrived(xbuf.at[src, 1], recv_x.at[src, 1], {"tp": other(t)})
            for hi in range(2):
                r = row_of(2 * src + hi)
                cols = pl.ds(hi * HEAD, HEAD)

                @pl.when(r != s)
                def _():
                    for at in which:
                        place = (kv.at[s, t, 0], kv.at[s, t, 1], qbuf.at[s])[at]
                        sem_a = recv_a.at[n_sp] if at == 2 else recv_a.at[s]
                        remote(xbuf.at[src, at, whole, cols], place, send_a.at[at], sem_a, {"sp": r}).start()
                    if 2 in which:
                        remote(xf.at[src, hi], fbuf.at[s], send_a.at[3], recv_a.at[n_sp + 1], {"sp": r}).start()

    third = w_ref.shape[0] // 3
    on_ring = w_ref.shape[0] // 32 * 16 + 16
    ringed = pl.ds(pl.multiple_of(parity * (3 * third - on_ring), 16), on_ring)
    shared = pl.ds(pl.multiple_of(parity * on_ring, 16), 3 * third - on_ring)
    half_way = n_sp // 2

    def chunk(d):
        return lax.rem(s + d + n_sp, n_sp)

    def pass_on(k, src, chunk_at, to, way):
        remote(src, wbuf.at[chunk_at, ringed], send_w.at[way, k], recv_w.at[way, k], to).start()

    def tick(k):
        here = chunk(-k)
        arrived(wbuf.at[here, ringed], recv_w.at[0, k - 1], to_last)

        @pl.when(k < half_way)
        def _():
            pass_on(k, wbuf.at[here, ringed], here, to_next, 0)

        piece = wbuf.at[here, shared]
        remote(piece, piece, send_y, recv_y, to_pair).start()

        @pl.when(k < half_way)
        def _():
            far = chunk(k)
            arrived(wbuf.at[far, ringed], recv_w.at[1, k - 1], to_next)

            @pl.when(k < half_way - 1)
            def _():
                pass_on(k, wbuf.at[far, ringed], far, to_last, 1)

            piece = wbuf.at[far, shared]
            remote(piece, piece, send_y, recv_y, to_pair).start()

    own_copy = pltpu.make_async_copy(w_ref, wbuf.at[s], own_sem)
    own_copy.start()
    pass_on(0, w_ref.at[ringed], s, to_next, 0)
    pass_on(0, w_ref.at[ringed], s, to_last, 1)
    scatter((0, 1))
    scatter((2,))
    deliver((0, 1))
    tick(1)
    deliver((2,))

    to_left, to_right, to_other = {"tp": left}, {"tp": right}, {"tp": other(t)}

    per_turn = n_sp // n_tp

    def at_step(owner, j):
        return lax.rem(source - owner - j // per_turn + 2 * n_tp, n_tp) + n_tp * lax.rem(j, per_turn)

    def stage_one(j):
        b = at_step(t, j)
        arrived(kv.at[b, t], recv_a.at[b], to_other)
        piece = kv.at[b, t]
        remote(piece, piece, send_b.at[0], recv_b.at[0, b], to_right).start()
        remote(piece, piece, send_b.at[1], recv_b.at[1, b], to_left).start()
        remote(piece, piece, send_b.at[2], recv_c.at[0], to_other).start()

    def stage_two(j):
        b = at_step(left, j)
        arrived(kv.at[b, left], recv_b.at[0, b], to_left)
        piece, half = kv.at[b, left], kv.at[b, left, 0]
        remote(half, half, send_b.at[3], recv_b.at[2, b], to_right).start()
        remote(piece, piece, send_c.at[0], recv_c.at[1], to_other).start()
        b = at_step(right, j)
        arrived(kv.at[b, right], recv_b.at[1, b], to_right)
        piece, half = kv.at[b, right], kv.at[b, right, 1]
        remote(half, half, send_b.at[4], recv_b.at[3, b], to_left).start()
        remote(piece, piece, send_c.at[1], recv_c.at[2], to_other).start()

    def stage_three(j):
        b = at_step(opp, j)
        for i, (way, device) in enumerate(((2, to_left), (3, to_right))):
            half = kv.at[b, opp, i]
            arrived(half, recv_b.at[way, b], device)
            remote(half, half, send_c.at[2 + i], recv_c.at[3 + i], to_other).start()

    lag = 2

    @pl.loop(0, n_sp + 2 * lag)
    def _(j):
        @pl.when(j < n_sp)
        def _():
            stage_one(j)

        @pl.when(jnp.logical_and(j >= lag, j < n_sp + lag))
        def _():
            stage_two(j - lag)

        @pl.when(j >= 2 * lag)
        def _():
            stage_three(j - 2 * lag)

        @pl.when(jnp.logical_and(j > 0, lax.rem(j, 8) == 0))
        def _():
            tick(j // 8 + 1)

    arrived(kv.at[:, other(t)], recv_c.at[0], to_other)
    arrived(kv.at[:, other(left)], recv_c.at[1], to_other)
    arrived(kv.at[:, other(right)], recv_c.at[2], to_other)
    arrived(kv.at[:, other(opp), 0], recv_c.at[3], to_other)
    arrived(kv.at[:, other(opp), 1], recv_c.at[4], to_other)
    arrived(qbuf, recv_a.at[n_sp], to_other)
    arrived(fbuf, recv_a.at[n_sp + 1], to_other)

    width = n_tp * sub

    @pl.loop(0, n_sp)
    def _(b):
        rows = kv[b, :, 0].reshape(width, HEAD).astype(jnp.float32)
        kn[b] = normed(rows, kg_ref[...]).astype(jnp.bfloat16)

    tick(4)
    group = 4
    tall, wide = group * sub, group * width
    factor = LOG2E / math.sqrt(HEAD)

    def bias_row(c, base):
        parts = []
        for b in range(group):
            slab = fbuf[c * group + b]
            for lane in range(width // HEAD):
                parts.append(slab[lane : lane + 1])
        return (base - jnp.concatenate(parts, axis=1)) * LOG2E

    @pl.loop(0, n_sp // group)
    def _(step):
        i = lax.rem(s + step, n_sp // group)

        @pl.when(step == 2)
        def _():
            tick(5)

        q = qbuf[pl.ds(i * group, group)].reshape(tall, HEAD).astype(jnp.float32)
        q = normed(q, qg_ref[...]).astype(jnp.bfloat16)
        base = fbuf[i * group, 0:1, 0:1]

        def visit(c, state, masked):
            top, total, acc = state
            keys = kn[pl.ds(c * group, group)].reshape(wide, HEAD)
            scores = lax.dot_general(q, keys, (((1,), (1,)), ((), ())), preferred_element_type=jnp.float32)
            scores = scores * factor + bias_row(c, base)
            if masked:
                line = lax.broadcasted_iota(jnp.int32, (tall, wide), 0)
                place = (line // sub) * width + t * sub + lax.rem(line, sub)
                scores = jnp.where(lax.broadcasted_iota(jnp.int32, (tall, wide), 1) <= place, scores, LOW)
            high = jnp.maximum(top, jnp.max(scores, axis=1, keepdims=True))
            raised = jnp.exp2(scores - high)
            shrink = jnp.exp2(top - high)
            total = total * shrink + jnp.sum(raised, axis=1, keepdims=True)
            vals = kv[pl.ds(c * group, group), :, 1].reshape(wide, HEAD)
            acc = acc * shrink + jnp.dot(raised.astype(jnp.bfloat16), vals, preferred_element_type=jnp.float32)
            return high, total, acc

        state = (
            jnp.full((tall, 1), LOW, jnp.float32),
            jnp.zeros((tall, 1), jnp.float32),
            jnp.zeros((tall, HEAD), jnp.float32),
        )
        state = visit(i, state, True)
        _, total, acc = lax.fori_loop(0, i, lambda c, st: visit(c, st, False), state)
        obuf[pl.ds(i * group, group)] = (acc / total).astype(jnp.bfloat16).reshape(group, sub, HEAD)

        @pl.loop(0, group)
        def _(n):
            r = i * group + n
            cols = pl.ds(pl.multiple_of(my_head * HEAD, HEAD), HEAD)

            @pl.when(r != s)
            def _():
                remote(obuf.at[r], att.at[t, :, cols], send_o.at[r], recv_o, {"sp": r, "tp": t}).start()

            @pl.when(r == s)
            def _():
                att[t, :, cols] = obuf[r]

    def o_wait(r):
        @pl.when(r != s)
        def _():
            left_over(obuf.at[r], send_o.at[r], {"sp": r, "tp": t})

    pl.loop(0, n_sp)(o_wait)
    tick(6)
    arrived(att.at[t, :, pl.ds(0, (n_sp - 1) * HEAD)], recv_o, to_other)

    row_gather(row, att, send_g.at[0], recv_g.at[0], lambda: tick(7))
    total_rows = n_tp * sub
    span = 256

    @pl.loop(0, total_rows // span)
    def _(m):
        rows = pl.ds(m * span, span)
        lhs = att[pl.ds(m * (span // sub), span // sub)].reshape(span, att.shape[2])
        product = jnp.dot(lhs, ow_ref[...], preferred_element_type=jnp.float32)
        mid[t, rows] = (res_ref[rows].astype(jnp.float32) + product).astype(jnp.bfloat16)

    row_gather(row, mid, send_g.at[1], recv_g.at[1], lambda: tick(8))
    cols = mid.shape[2]
    rows = mid.shape[1]
    core = row.core
    depth = wbuf.shape[2]
    span = 128

    @pl.loop(0, rows // span)
    def _(m):
        at = pl.ds(m * span, span)
        blocks = [mid[u, at].astype(jnp.float32) for u in range(n_tp)]
        square = sum(jnp.sum(b * b, axis=1, keepdims=True) for b in blocks) / (n_tp * cols)
        scale = lax.rsqrt(square + EPS)
        for u in range(n_tp):
            nrm[at, pl.ds(u * cols, cols)] = (blocks[u] * scale * gain_ref[u]).astype(jnp.bfloat16)

    own_copy.wait()
    arrived(wbuf.at[pl.ds(0, n_sp - 1), shared], recv_y, to_pair)

    def stacked(which, first, count):
        return jnp.concatenate([wbuf[first + z, pl.ds(which * third, third)] for z in range(count)], axis=1)

    tall = 256

    @pl.loop(0, rows // tall)
    def _(m):
        at = pl.ds(m * tall, tall)
        across = (((1,), (1,)), ((), ()))
        gate = lax.dot_general(nrm[at], stacked(0, 0, n_sp), across, preferred_element_type=jnp.float32)
        up = lax.dot_general(nrm[at], stacked(1, 0, n_sp), across, preferred_element_type=jnp.float32)
        hid[at] = (gate / (1.0 + jnp.exp(-gate)) * up).astype(jnp.bfloat16)

    chips = (opp, right, left, t)

    def add(k):
        arrived(pair.at[k], recv_p.at[k], to_other)
        mine = part[k, core].astype(jnp.float32) + pair[k].astype(jnp.float32)
        if k < 3:
            total[k] = mine.astype(jnp.bfloat16)
            remote(total.at[k], landed.at[k], send_r.at[k], recv_r.at[k], {"tp": chips[k]}).start()
            return None
        return mine

    for k in range(4):
        each = cols // depth
        for side in range(2):
            down = stacked(2, (chips[k] - core + side) * each, each)
            part[k, side] = jnp.dot(hid[...], down, preferred_element_type=jnp.float32).astype(jnp.bfloat16)
        remote(part.at[k, 1 - core], pair.at[k], send_p.at[k], recv_p.at[k], to_other).start()
        if k > 0:
            add(k - 1)
    mine = add(3) + mid[t].astype(jnp.float32)
    for k in (1, 2, 0):
        arrived(landed.at[k], recv_r.at[k], to_other)
        mine = mine + landed[k].astype(jnp.float32)
    out_ref[...] = mine.astype(jnp.bfloat16)
    for k in range(4):
        left_over(part.at[k, 1 - core], send_p.at[k], to_other)
    for k in range(3):
        left_over(total.at[k], send_r.at[k], {"tp": chips[k]})
    for at, ref in enumerate((k_ref, v_ref, q_ref)):
        left_over(ref.at[pl.ds(0, (n_tp - 1) * sub)], send_x.at[at], to_other)
        left_over(qbuf.at[pl.ds(0, n_sp - 1)], send_a.at[at], to_other)
    left_over(xf.at[pl.ds(0, n_tp - 1)], send_x.at[3], to_other)
    left_over(fbuf.at[pl.ds(0, n_sp - 1)], send_a.at[3], to_other)

    @pl.when(own)
    def _():
        for at in range(3):
            left_over(qbuf.at[pl.ds(0, n_tp - 1)], send_d.at[at], to_other)
        left_over(fbuf.at[pl.ds(0, n_tp - 1)], send_d.at[3], to_other)

    left_over(kv.at[:, t], send_b.at[0], to_right)
    left_over(kv.at[:, t], send_b.at[1], to_left)
    left_over(kv.at[:, t], send_b.at[2], to_other)
    left_over(kv.at[:, left, 0], send_b.at[3], to_right)
    left_over(kv.at[:, right, 1], send_b.at[4], to_left)
    left_over(kv.at[:, left], send_c.at[0], to_other)
    left_over(kv.at[:, right], send_c.at[1], to_other)
    left_over(kv.at[:, opp, 0], send_c.at[2], to_other)
    left_over(kv.at[:, opp, 1], send_c.at[3], to_other)
    for k in range(half_way):
        left_over(wbuf.at[s, ringed], send_w.at[0, k], to_next)
    for k in range(half_way - 1):
        left_over(wbuf.at[s, ringed], send_w.at[1, k], to_last)
    left_over(wbuf.at[pl.ds(0, n_sp - 1), shared], send_y, to_pair)


def local(n_sp, n_tp, q, k, v, f, res, qg, kg, ow, ng, gw, uw, dw):
    rows, cols = q.shape
    sub = rows // n_tp
    hbm = pl.BlockSpec(memory_space=pltpu.HBM)
    vmem = pl.BlockSpec(memory_space=pltpu.VMEM)
    dma = pltpu.SemaphoreType.DMA
    flat = jnp.concatenate((gw, uw, dw), axis=1).T
    f = jnp.pad(f.T.reshape(2, rows // HEAD, HEAD), ((0, 0), (0, 8 - rows // HEAD), (0, 0)))
    bf = jnp.bfloat16
    width = n_sp * HEAD
    ff = gw.shape[1]
    return pl.pallas_call(
        functools.partial(layer_kernel, n_sp, n_tp),
        out_shape=jax.ShapeDtypeStruct((rows, cols), bf),
        in_specs=[hbm] * 4 + [vmem] * 4 + [hbm, vmem],
        out_specs=vmem,
        scratch_shapes=[
            pltpu.VMEM((n_sp, sub, HEAD), bf),
            pltpu.VMEM((n_sp, n_tp, 2, sub, HEAD), bf),
            pltpu.VMEM((n_sp, 8, HEAD), jnp.float32),
            pltpu.VMEM((n_sp, rows, HEAD), bf),
            pltpu.VMEM((n_sp, sub, HEAD), bf),
            pltpu.VMEM((n_tp, sub, width), bf),
            pltpu.VMEM((n_tp, rows, cols), bf),
            dma((4,)),
            dma((n_sp + 2,)),
            dma((5,)),
            dma((4, n_sp)),
            dma((4,)),
            dma((5,)),
            dma((n_sp,)),
            dma,
            dma((2, 9)),
            dma((2, 9)),
            pltpu.VMEM((n_sp, 3 * ff, gw.shape[0]), bf),
            pltpu.VMEM((rows, n_tp * cols), bf),
            pltpu.VMEM((rows, ff), bf),
            pltpu.VMEM((4, 2, rows, cols), bf),
            pltpu.VMEM((4, rows, cols), bf),
            pltpu.VMEM((3, rows, cols), bf),
            pltpu.VMEM((3, rows, cols), bf),
            pltpu.VMEM((n_tp, 3, sub, cols), bf),
            pltpu.VMEM((n_tp, 2, 8, HEAD), jnp.float32),
            dma((4,)),
            dma((n_tp, 4)),
            dma((4,)),
            dma,
            dma((2, n_sp // 2)),
            dma((2, n_sp // 2)),
            dma,
            dma,
            dma((4,)),
            dma((4,)),
            dma((3,)),
            dma((3,)),
        ],
        compiler_params=pltpu.CompilerParams(
            collective_id=0, has_side_effects=True, vmem_limit_bytes=60 * 1024 * 1024
        ),
        cost_estimate=pl.CostEstimate(flops=40_000_000_000, bytes_accessed=100_000_000, transcendentals=0),
        name="layer",
    )(q, k, v, f, res, ow, qg.reshape(1, HEAD), kg.reshape(1, HEAD), flat, ng.reshape(n_tp, 1, cols))


def solution(mesh):
    whole = P(("grp", "sp"), "tp")
    weight = P("sp", "tp")
    placed = (whole,) * 5 + (P(), P(), P(None, "tp"), P(), weight, weight, weight)
    return jax.shard_map(
        functools.partial(local, mesh.shape["sp"], mesh.shape["tp"]),
        mesh=mesh,
        in_specs=placed,
        out_specs=whole,
        check_vma=False,
    )
```
